256 devices in a mesh: grp: 2 (over y), ep: 64 (over z, x), tp: 2 (over core).
Axes of the slice: x: 4, y: 2, z: 16, core: 2. Of those that a mesh axis runs over, the one named last changes fastest.
The devices are a block of a 4x16x16 slice.
Arguments:
- tokens: bfloat16 [12288, 2048], P(('grp', 'ep')), parts along dimension 0, may hold values from -6 to 6
- prior_state: float32 [2, 12288, 4096], P(None, ('grp', 'ep'), 'tp'), parts along dimension 1, may hold values from -6 to 6
- mix_gain: float32 [2048], replicated, may hold values from 0.1 to 1.9
- in_weight: bfloat16 [2048, 1024], P(None, 'tp'), may hold values from -0.125 to 0.125
- decay_rate: float32 [64, 64], P('tp'), may hold values from 0.2 to 20
- frequency: float32 [64, 64], P('tp'), may hold values from 0 to 12
- log_step: float32 [64], P('tp'), may hold values from -4.6 to 0
- input_map: float32 [2, 64, 64, 16], P(None, 'tp'), may hold values from -6 to 6
- output_map: float32 [2, 64, 16, 64], P(None, 'tp'), may hold values from -0.5 to 0.5
- skip_gain: float32 [1024], P('tp'), may hold values from -4 to 4
- out_weight: bfloat16 [1024, 2048], P('tp'), may hold values from -0.1875 to 0.1875
- channel_gain: float32 [2048], replicated, may hold values from 0.1 to 1.9
- expert_gate: bfloat16 [64, 2048, 512], P('ep', None, 'tp'), may hold values from -0.125 to 0.125
- expert_up: bfloat16 [64, 2048, 512], P('ep', None, 'tp'), may hold values from -0.125 to 0.125
- expert_down: bfloat16 [64, 512, 2048], P('ep', 'tp'), may hold values from -0.25 to 0.25
- shared_gate: bfloat16 [2048, 512], P(None, 'tp'), may hold values from -0.125 to 0.125
- shared_up: bfloat16 [2048, 512], P(None, 'tp'), may hold values from -0.125 to 0.125
- shared_down: bfloat16 [512, 2048], P('tp'), may hold values from -0.25 to 0.25
- routes: int32 [12288, 6], P(('grp', 'ep')), parts along dimension 0, may hold values from 0 to 63, all different within a row; in each aligned block of 96 rows (0 to 95, 96 to 191, ...) at most 13 rows name the same one
- route_weights: float32 [12288, 6], P(('grp', 'ep')), parts along dimension 0, may hold values from 0.05 to 0.8
Outputs:
- layer_out: bfloat16 [12288, 2048], P(('grp', 'ep'), 'tp'), parts along dimension 0
- new_state: float32 [2, 12288, 4096], P(None, ('grp', 'ep'), 'tp'), parts along dimension 1
The draws below stay inside these ranges and needn't reach their ends.
There are 2 independent parts, one for each index of `grp`. The reference program is written for one: setup_inputs(seed, part) draws one part's arguments, and reference() takes and returns one part's arrays. A program takes and returns all parts, laid end to end along the dimension named above; an argument that names none is the same for every part. Nothing has to cross between parts.
Inputs may be any that keep to these rules, and one draw needn't show every extreme that they name: `routes`: each row names 6 different experts; among the rows of one index of ep no expert is named by more than 13 rows.
All inputs are finite; a program needn't handle non-finite values.
Results may differ from the reference program's by a relative error of at most 0.017.
Values may be sent and summed in bfloat16 or wider, within the bound.
A program may use at most 128 MiB of HBM per device.

```python
import math
import jax
import jax.numpy as jnp
import numpy as np
from jax import lax

D = 2048
SSM_WIDTH = 1024
GROUPS = 64
GROUP_WIDTH = 16
STATE = 64
EXP_WIDTH = 512
SHARED_WIDTH = 512
TOPK = 6
SEQ_DEV = 96
SEQS = 6144
EXPERTS = 64
CAP = 13
N_EP = 64
N_TP = 2


def block_levels(stream_key, extent, pieces, smallest, high):
    def one(position, blocks):
        heights = jax.random.uniform(jax.random.fold_in(jax.random.fold_in(stream_key, 6), position), (blocks,), jnp.float32, smallest / len(pieces), high / len(pieces))
        return jnp.repeat(jnp.exp(heights), extent[position] // blocks).reshape((-1,) + (1,) * (len(extent) - position - 1))

    factor_of = one(*pieces[0])
    for cut in pieces[1:]:
        factor_of = factor_of * one(*cut)
    return factor_of


def deal_out(rng, own, number, rows, number_of, top, reach, skew):
    order = jax.random.permutation(rng, number_of)
    packed, ordinary = shares(number_of, rows * top, reach, skew, True), shares(number_of, rows * top, reach, skew, False)
    places = jnp.arange(number_of)

    def named(sizes, offset_by):
        used = int((sizes > 0).sum())
        fixed = max(1, used // 4)
        passed = fixed + (places - fixed + offset_by * (used - fixed)) % max(1, number_of - fixed)
        return jnp.zeros((number_of,), jnp.int32).at[order[jnp.where(places < fixed, places, passed)]].set(jnp.asarray(sizes, jnp.int32))

    sizes = jnp.where(number % 4 == 0, named(packed, number // 4), named(ordinary, number - number // 4 - 1))
    mixed = jax.random.permutation(jax.random.fold_in(own, 3), number_of)
    donor, receiver = mixed[0:number_of // 2 * 2:2], mixed[1:number_of // 2 * 2:2]
    margin = jnp.minimum(sizes[donor] - 1, reach - sizes[receiver]) // 2
    margin = jnp.where((donor == order[0]) | (receiver == order[0]) | (sizes[receiver] == 0), 0, jnp.maximum(margin, 0))
    passed = jax.random.randint(jax.random.fold_in(own, 4), (number_of // 2,), 0, 1 << 20) % (margin + 1)
    sizes = sizes.at[donor].add(-passed).at[receiver].add(passed)
    labels = jnp.searchsorted(jnp.cumsum(sizes), jnp.arange(rows * top), side="right").astype(jnp.int32)
    grid = labels.reshape(top, rows).T
    grid = grid[jax.random.permutation(jax.random.fold_in(own, 1), rows)]
    offset_by = jax.random.randint(jax.random.fold_in(own, 2), (rows, 1), 0, top)
    return jnp.take_along_axis(grid, (jnp.arange(top)[None, :] + offset_by) % top, axis=1)


def shares(amount, total, reach, slope, full):
    weights = [(1 << 20) // math.isqrt(rank ** slope) + 1 for rank in range(1, amount + 1)]
    largest = reach if full else min(reach, max(-(-total // amount), total * weights[0] // sum(weights)))
    least = 1 if total - largest >= amount - 1 else 0
    counts, spare = [largest] + [least] * (amount - 1), total - largest - least * (amount - 1)
    while spare > 0:
        free = [i for i in range(1, amount) if counts[i] < largest] or [i for i in range(1, amount) if counts[i] < reach]
        mass, left = sum([weights[i] for i in free]), spare
        for i in free:
            more = min(reach - counts[i], max(1, left * weights[i] // mass), spare)
            counts[i] = counts[i] + more
            spare = spare - more
    return np.array(counts)


def gaussian(key, dims, spread, most, shards=(), held_as=jnp.bfloat16):
    drawn = spread * jax.random.normal(key, dims, jnp.float32)
    if shards:
        drawn = drawn * block_levels(key, dims, shards, -0.22, 0.18)
    return jnp.clip(drawn, -most, most).astype(held_as)


def setup_inputs(seed: int = 0, part: int = 0) -> dict:
    keys = jax.random.split(jax.random.key(seed), 21)
    part_keys = jax.random.split(jax.random.fold_in(keys[20], part), 21)
    tokens = gaussian(part_keys[0], (SEQS, D), 1.0, 6.0, ((0, 64),))
    prior_state = gaussian(part_keys[1], (2, SEQS, GROUPS * STATE), 1.0, 6.0, ((1, 64), (2, 2)), jnp.float32)
    mix_gain = jnp.clip(1.0 + 0.18 * jax.random.normal(keys[2], (D,), jnp.float32), 0.1, 1.9)
    in_weight = gaussian(keys[3], (D, SSM_WIDTH), D ** -0.5, 0.125, ((1, 2),))
    decay_rate = jnp.clip(jnp.exp(math.log(20.0) - 4.6051702 * jax.random.uniform(keys[4], (GROUPS, STATE), jnp.float32) ** block_levels(keys[4], (GROUPS, STATE), ((0, 2),), -0.2, 0.2)), 0.2, 20.0)
    frequency = jnp.clip(12.0 * jax.random.uniform(keys[5], (GROUPS, STATE), jnp.float32) ** block_levels(keys[5], (GROUPS, STATE), ((0, 2),), -0.2, 0.2), 0.0, 12.0)
    log_step = jnp.clip(-4.6 + 4.6 * jax.random.uniform(keys[6], (GROUPS,), jnp.float32) ** block_levels(keys[6], (GROUPS,), ((0, 2),), -0.2, 0.2), -4.6, 0.0)
    input_map = gaussian(keys[7], (2, GROUPS, STATE, GROUP_WIDTH), 1.0, 6.0, ((1, 2),), jnp.float32)
    output_map = gaussian(keys[8], (2, GROUPS, GROUP_WIDTH, STATE), (2 * STATE) ** -0.5, 0.5, ((1, 2),), jnp.float32)
    skip_gain = gaussian(keys[9], (SSM_WIDTH,), 1.0, 4.0, ((0, 2),), jnp.float32)
    out_weight = gaussian(keys[10], (SSM_WIDTH, D), SSM_WIDTH ** -0.5, 0.1875, ((0, 2),))
    channel_gain = jnp.clip(1.0 + 0.18 * jax.random.normal(keys[11], (D,), jnp.float32), 0.1, 1.9)
    expert_gate = gaussian(keys[12], (EXPERTS, D, EXP_WIDTH), D ** -0.5, 0.125, ((0, 64), (2, 2)))
    expert_up = gaussian(keys[13], (EXPERTS, D, EXP_WIDTH), D ** -0.5, 0.125, ((0, 64), (2, 2)))
    expert_down = gaussian(keys[14], (EXPERTS, EXP_WIDTH, D), EXP_WIDTH ** -0.5, 0.25, ((0, 64), (1, 2)))
    shared_gate = gaussian(keys[15], (D, SHARED_WIDTH), D ** -0.5, 0.125, ((1, 2),))
    shared_up = gaussian(keys[16], (D, SHARED_WIDTH), D ** -0.5, 0.125, ((1, 2),))
    shared_down = gaussian(keys[17], (SHARED_WIDTH, D), SHARED_WIDTH ** -0.5, 0.25, ((0, 2),))
    routes_keys = jax.random.split(jax.random.fold_in(part_keys[18], 1), SEQS // SEQ_DEV)
    routes_turns = jax.random.permutation(jax.random.fold_in(part_keys[18], 3), SEQS // SEQ_DEV)
    routes = jax.vmap(lambda own, number: deal_out(jax.random.fold_in(part_keys[18], 2), own, number, SEQ_DEV, EXPERTS, TOPK, CAP, 2))(routes_keys, routes_turns).reshape((SEQS, TOPK))
    route_weights = jnp.clip(0.05 + 0.75 * jax.random.uniform(part_keys[19], (SEQS, TOPK), jnp.float32) ** block_levels(part_keys[19], (SEQS, TOPK), ((0, 64),), -0.2, 0.2), 0.05, 0.8)
    return {"tokens": tokens, "prior_state": prior_state, "mix_gain": mix_gain, "in_weight": in_weight, "decay_rate": decay_rate, "frequency": frequency, "log_step": log_step, "input_map": input_map, "output_map": output_map, "skip_gain": skip_gain, "out_weight": out_weight, "channel_gain": channel_gain, "expert_gate": expert_gate, "expert_up": expert_up, "expert_down": expert_down, "shared_gate": shared_gate, "shared_up": shared_up, "shared_down": shared_down, "routes": routes, "route_weights": route_weights}


norm_eps = 1e-06
highest = lax.Precision.HIGHEST

def root_scale(activations, scale_gain):
    values = activations.astype(jnp.float32)
    factor = lax.rsqrt(lax.optimization_barrier(jnp.mean(values * values, axis=-1, keepdims=True)) + norm_eps)
    return (values * factor * scale_gain).astype(jnp.bfloat16)

def state_update(drive_rows, prior_state, decay_rate, frequency, log_step, input_map, output_map, skip_gain):
    sequences = drive_rows.shape[0]
    groups = decay_rate.shape[0]
    driven = drive_rows.astype(jnp.float32).reshape(sequences, groups, -1)
    step_size = jnp.exp(log_step)[:, None]
    real_rate = -decay_rate
    magnitude = jnp.exp(real_rate * step_size)
    turn_real = magnitude * jnp.cos(frequency * step_size)
    turn_imag = magnitude * jnp.sin(frequency * step_size)
    denominator = real_rate * real_rate + frequency * frequency
    hold_real = ((turn_real - 1.0) * real_rate + turn_imag * frequency) / denominator
    hold_imag = (turn_imag * real_rate - (turn_real - 1.0) * frequency) / denominator
    push_real = jnp.einsum('sgh,gph->sgp', driven, input_map[0], precision=highest)
    push_imag = jnp.einsum('sgh,gph->sgp', driven, input_map[1], precision=highest)
    enter_real = push_real * hold_real - push_imag * hold_imag
    enter_imag = push_real * hold_imag + push_imag * hold_real
    old_real = prior_state[0].reshape(sequences, groups, -1)
    old_imag = prior_state[1].reshape(sequences, groups, -1)
    fresh_real = turn_real * old_real - turn_imag * old_imag + enter_real
    fresh_imag = turn_real * old_imag + turn_imag * old_real + enter_imag
    readout = jnp.einsum('ghp,sgp->sgh', output_map[0], fresh_real, precision=highest)
    readout = readout - jnp.einsum('ghp,sgp->sgh', output_map[1], fresh_imag, precision=highest)
    readout = readout.reshape(sequences, -1) + skip_gain * drive_rows.astype(jnp.float32)
    fresh = jnp.stack([fresh_real.reshape(sequences, -1), fresh_imag.reshape(sequences, -1)])
    return (readout, fresh)

def split_block(activations, gate_weight, up_weight, down_weight):
    col_width = gate_weight.shape[1] // N_TP
    summed = jnp.zeros((activations.shape[0], down_weight.shape[1]), jnp.float32)
    for portion in range(N_TP):
        lower = portion * col_width
        gate_val = jnp.dot(activations, gate_weight[:, lower:lower + col_width], preferred_element_type=jnp.float32)
        up_val = jnp.dot(activations, up_weight[:, lower:lower + col_width], preferred_element_type=jnp.float32)
        hidden = (jax.nn.silu(gate_val) * up_val).astype(jnp.bfloat16)
        piece = jnp.dot(hidden, down_weight[lower:lower + col_width], preferred_element_type=jnp.float32)
        summed = summed + lax.optimization_barrier(piece.astype(jnp.bfloat16)).astype(jnp.float32)
    return summed

def reference(tokens, prior_state, mix_gain, in_weight, decay_rate, frequency, log_step, input_map, output_map, skip_gain, out_weight, channel_gain, expert_gate, expert_up, expert_down, shared_gate, shared_up, shared_down, routes, route_weights):
    normed = root_scale(tokens, mix_gain)
    drive_rows = jnp.dot(normed, in_weight, preferred_element_type=jnp.float32).astype(jnp.bfloat16)
    readout, new_state = state_update(drive_rows, prior_state, decay_rate, frequency, log_step, input_map, output_map, skip_gain)
    activated = jax.nn.gelu(readout).astype(jnp.bfloat16)
    col_width = out_weight.shape[0] // N_TP
    mixer_out = jnp.zeros((SEQS, D), jnp.float32)
    for portion in range(N_TP):
        lower = portion * col_width
        piece = jnp.dot(activated[:, lower:lower + col_width], out_weight[lower:lower + col_width], preferred_element_type=jnp.float32)
        mixer_out = mixer_out + lax.optimization_barrier(piece.astype(jnp.bfloat16)).astype(jnp.float32)
    middle = (tokens.astype(jnp.float32) + mixer_out).astype(jnp.bfloat16)
    second_normed = root_scale(middle, channel_gain)
    shared_out = split_block(second_normed, shared_gate, shared_up, shared_down)
    slot_limit = N_EP * CAP
    flat_routes = routes.reshape(-1)
    flat_weights = route_weights.reshape(-1)

    def one_expert(running, operands):
        expert_id, gate_weight, up_weight, down_weight = operands
        matched = flat_routes == expert_id
        chosen = jnp.nonzero(matched, size=slot_limit, fill_value=0)[0].astype(jnp.int32)
        found_count = jnp.sum(matched.astype(jnp.int32))
        is_valid = jnp.arange(slot_limit, dtype=jnp.int32) < found_count
        row_index = chosen // TOPK
        picked_rows = jnp.take(second_normed, row_index, axis=0)
        produced = split_block(picked_rows, gate_weight, up_weight, down_weight).astype(jnp.bfloat16)
        produced = lax.optimization_barrier(produced).astype(jnp.float32)
        weight_vals = jnp.where(is_valid, jnp.take(flat_weights, chosen), jnp.zeros_like(flat_weights[:1]))
        running = running.at[row_index].add(weight_vals[:, None] * produced)
        return (running, None)
    routed, _ = lax.scan(one_expert, jnp.zeros((SEQS, D), jnp.float32), (jnp.arange(EXPERTS, dtype=jnp.int32), expert_gate, expert_up, expert_down))
    layer_out = (middle.astype(jnp.float32) + routed + shared_out).astype(jnp.bfloat16)
    return (layer_out, new_state)
```

```python
import functools

import jax
import jax.numpy as jnp
from jax import lax
from jax.experimental import pallas as pl
from jax.experimental.pallas import tpu as pltpu
from jax.sharding import PartitionSpec as P

MESH = pl.DeviceIdType.MESH
norm_eps = 1e-06
ROW_RING = 4
CHUNKS = 4
LANES = 128


def moe_kernel(
    cfg,
    tokens_ref,
    base_ref,
    table_ref,
    gate_hbm,
    up_hbm,
    down_hbm,
    out_ref,
    gathered,
    tables,
    codes,
    shares,
    pick,
    spread,
    staged,
    rows_in,
    w_in,
    w_out,
    partial,
    partner_part,
    total,
    back,
    sums_in,
    sums_out,
    w_sem,
    t_send,
    t_recv,
    z_send,
    z_recv,
    x_send,
    x_recv,
    c_send,
    c_recv,
    p_send,
    p_recv,
    b_send,
    b_recv,
    r_send,
    r_recv,
):
    Z, X, S, H, R, nc, top = cfg
    W = H // nc
    half = Z // 2
    F = gate_hbm.shape[2]
    ep = lax.axis_index("ep")
    tp = lax.axis_index("tp")
    other = 1 - tp
    z, x = ep // X, lax.rem(ep, X)

    def at_z(offset):
        return {"ep": lax.rem(z + offset + Z, Z) * X + x}

    def at_x(offset):
        return {"ep": z * X + lax.rem(x + offset + X, X)}

    partner = {"tp": other}

    def send(src, dst, s_sem, r_sem, device):
        return pltpu.make_async_remote_copy(
            src_ref=src, dst_ref=dst, send_sem=s_sem, recv_sem=r_sem,
            device_id=device, device_id_type=MESH,
        )

    def weight_copies():
        return (
            pltpu.make_async_copy(gate_hbm.at[0], w_in.at[:, pl.ds(0, F)], w_sem.at[0]),
            pltpu.make_async_copy(up_hbm.at[0], w_in.at[:, pl.ds(F, F)], w_sem.at[1]),
            pltpu.make_async_copy(down_hbm.at[0], w_out, w_sem.at[2]),
        )

    for copy in weight_copies():
        copy.start()

    barrier = pltpu.get_barrier_semaphore()
    for k in range(1, Z):
        pl.semaphore_signal(barrier, inc=1, device_id=at_z(k), device_id_type=MESH)
    for d in range(1, X):
        pl.semaphore_signal(barrier, inc=1, device_id=at_x(d), device_id_type=MESH)
    pl.semaphore_signal(barrier, inc=1, device_id=partner, device_id_type=MESH)

    tables[0] = table_ref[...]
    for c in range(nc):
        gathered[0, c] = tokens_ref[:, pl.ds(pl.multiple_of(tp * H + c * W, W), W)]

    pl.semaphore_wait(barrier, Z + X - 1)

    def table_copy(k):
        return send(table_ref, tables.at[k], t_send.at[k], t_recv.at[k], at_z(k))

    for k in range(1, Z):
        table_copy(k).start()

    def z_copy(way, k, c):
        if way == 0:
            return send(gathered.at[k, c], gathered.at[k + 1, c], z_send.at[0, k, c], z_recv.at[k + 1, c], at_z(1))
        r = lax.rem(Z - k, Z)
        return send(gathered.at[r, c], gathered.at[Z - k - 1, c], z_send.at[1, k, c], z_recv.at[Z - k - 1, c], at_z(-1))

    def z_limit(way, c):
        mine = (c < nc // 2) if way == 0 else (c >= nc // 2)
        return half if mine else half - 1

    def z_stage(k, c):
        for way in (0, 1):
            limit = z_limit(way, c)

            @pl.when((k >= 1) & (k <= limit))
            def _():
                z_copy(way, k - 1, c).wait_recv()

            @pl.when(k + 1 <= limit)
            def _():
                z_copy(way, k, c).start()

    for c in range(nc):
        z_stage(jnp.int32(0), c)

    for k in range(1, Z):
        table_copy(k).wait_recv()
    before = (
        lax.broadcasted_iota(jnp.int32, (LANES, LANES), 0) < lax.broadcasted_iota(jnp.int32, (LANES, LANES), 1)
    ).astype(jnp.float32).astype(jnp.bfloat16)
    for d in range(X):
        expert = (z * X + lax.rem(x + d, X)).astype(jnp.float32)
        named = jnp.zeros((Z, LANES), jnp.float32)
        weight = jnp.zeros((Z, LANES), jnp.float32)
        for k in range(top):
            hit = tables[:, k, :] == expert
            named = named + jnp.where(hit, 1.0, 0.0)
            weight = weight + jnp.where(hit, tables[:, 8 + k, :], 0.0)
        rank = jnp.dot(named.astype(jnp.bfloat16), before, preferred_element_type=jnp.float32)
        codes[d] = jnp.where(named > 0.0, rank, -1.0)
        shares[d] = weight

    def build(r, carry):
        slot = lax.broadcasted_iota(jnp.int32, (R, LANES), 0).astype(jnp.float32)
        parts, weighted = [], []
        for d in range(X):
            block = jnp.where(codes[d, pl.ds(r, 1), :] == slot, 1.0, 0.0)
            parts.append(block)
            weighted.append(block * shares[d, pl.ds(r, 1), :])
        pick[r] = jnp.concatenate(parts, axis=0).astype(jnp.bfloat16)
        spread[r] = jnp.concatenate(weighted, axis=0).T.astype(jnp.bfloat16)
        return carry

    lax.fori_loop(0, Z, build, 0)
    for copy in weight_copies():
        copy.wait()

    def x_copy(r, d):
        rows = pl.ds(d * R, R)
        return send(staged.at[r, :, rows, :], rows_in.at[r, tp, :, rows, :], x_send.at[r], x_recv.at[r], at_x(d))

    def c_copy(r):
        return send(rows_in.at[r, tp], rows_in.at[r, tp], c_send.at[r], c_recv.at[r], partner)

    def p_copy(r):
        return send(partial.at[r, other], partner_part.at[r], p_send.at[r], p_recv.at[r], partner)

    def b_copy(r, d):
        rows = pl.ds(d * R, R)
        return send(total.at[r, :, rows, :], back.at[r, :, rows, :], b_send.at[r], b_recv.at[r], at_x(-d))

    def select(r):
        for c in range(nc):
            chosen = jnp.dot(
                pick[r, :, pl.ds(0, S)], gathered[r, c], preferred_element_type=jnp.float32
            ).astype(jnp.bfloat16)
            rows_in[r, tp, c, pl.ds(0, R), :] = chosen[:R]
            staged[r, c] = chosen
        for d in range(1, X):
            x_copy(r, d).start()

    rest = pl.ds(R, (X - 1) * R)

    def hand_over(r):
        send(staged.at[r, :, rest, :], rows_in.at[r, tp, :, rest, :], x_send.at[r], x_recv.at[r], at_x(1)).wait_recv()
        c_copy(r).start()

    def expert(r):
        send(rows_in.at[r, other], rows_in.at[r, other], c_send.at[r], c_recv.at[r], partner).wait_recv()
        acc = jnp.zeros((X * R, 2 * F), jnp.float32)
        for h in range(2):
            for c in range(nc):
                acc = acc + jnp.dot(
                    rows_in[r, h, c], w_in[pl.ds(h * H + c * W, W), :], preferred_element_type=jnp.float32
                )
        hidden = (jax.nn.silu(acc[:, :F]) * acc[:, F:]).astype(jnp.bfloat16)
        for h in range(2):
            for c in range(nc):
                partial[r, h, c] = jnp.dot(
                    hidden, w_out[:, pl.ds(h * H + c * W, W)], preferred_element_type=jnp.float32
                ).astype(jnp.bfloat16)
        p_copy(r).start()

    def join(r):
        p_copy(r).wait_recv()
        for c in range(nc):
            y = (partial[r, tp, c].astype(jnp.float32) + partner_part[r, c].astype(jnp.float32)).astype(jnp.bfloat16)
            back[r, c, pl.ds(0, R), :] = y[:R]
            total[r, c] = y
        for d in range(1, X):
            b_copy(r, d).start()

    def of_pair(stage, k, way):
        if way == 0:
            @pl.when((k >= 0) & (k <= half))
            def _():
                stage(k)
        else:
            @pl.when((k >= 1) & (k < half))
            def _():
                stage(Z - k)

    def step(i, carry):
        z_stage(i, 0)
        of_pair(select, i - 1, 0)
        of_pair(select, i - 1, 1)
        z_stage(i, 1)
        of_pair(hand_over, i - 2, 0)
        of_pair(hand_over, i - 2, 1)
        of_pair(expert, i - 3, 0)
        z_stage(i, 2)
        of_pair(expert, i - 3, 1)
        of_pair(join, i - 4, 0)
        z_stage(i, 3)
        of_pair(join, i - 4, 1)
        return carry

    lax.fori_loop(1, half + 5, step, 0)

    def r_copy(way, k, c):
        if way == 0:
            return send(sums_out.at[k, c], sums_in.at[k - 1, c], r_send.at[k, c], r_recv.at[k - 1, c], at_z(-1))
        return send(sums_out.at[Z - k, c], sums_in.at[Z - k + 1, c], r_send.at[Z - k, c], r_recv.at[Z - k + 1, c], at_z(1))

    def share_of(r, c):
        return jnp.dot(spread[r, pl.ds(0, S), :], back[r, c], preferred_element_type=jnp.float32)

    def back_wait(r):
        send(total.at[r, :, rest, :], back.at[r, :, rest, :], b_send.at[r], b_recv.at[r], at_x(1)).wait_recv()

    def go_back(i, carry):
        k = half - i
        back_wait(k)

        @pl.when(k < half)
        def _():
            back_wait(Z - k)

        for c in range(nc):
            for way in (0, 1):
                limit = z_limit(way, c)
                r = k if way == 0 else Z - k

                @pl.when(k <= limit)
                def _():
                    mine = share_of(r, c)

                    @pl.when(k == limit)
                    def _():
                        sums_out[r, c] = mine.astype(jnp.bfloat16)

                    @pl.when(k < limit)
                    def _():
                        r_copy(way, k + 1, c).wait_recv()
                        sums_out[r, c] = (mine + sums_in[r, c].astype(jnp.float32)).astype(jnp.bfloat16)

                    r_copy(way, k, c).start()
        return carry

    lax.fori_loop(0, half, go_back, 0)

    back_wait(0)
    for c in range(nc):
        mine = share_of(0, c) + base_ref[:, pl.ds(c * W, W)]
        r_copy(0, 1, c).wait_recv()
        r_copy(1, 1, c).wait_recv()
        mine = mine + sums_in[0, c].astype(jnp.float32) + sums_in[Z, c].astype(jnp.float32)
        out_ref[:, pl.ds(c * W, W)] = mine.astype(out_ref.dtype)

    for k in range(1, Z):
        table_copy(k).wait_send()

    def drain(k, carry):
        for c in range(nc):
            for way in (0, 1):
                limit = z_limit(way, c)

                @pl.when(k + 1 <= limit)
                def _():
                    z_copy(way, k, c).wait_send()
                    r_copy(way, k + 1, c).wait_send()
        return carry

    lax.fori_loop(0, half, drain, 0)

    def drain_rows(r, carry):
        send(staged.at[r, :, rest, :], rows_in.at[r, tp, :, rest, :], x_send.at[r], x_recv.at[r], at_x(1)).wait_send()
        c_copy(r).wait_send()
        p_copy(r).wait_send()
        send(total.at[r, :, rest, :], back.at[r, :, rest, :], b_send.at[r], b_recv.at[r], at_x(1)).wait_send()
        return carry

    lax.fori_loop(0, Z, drain_rows, 0)


def moe(tokens, base, table, gate, up, down, top):
    S, D = tokens.shape
    H = D // lax.axis_size("tp")
    X = ROW_RING
    Z = lax.axis_size("ep") // X
    nc = CHUNKS
    W = H // nc
    R = 16
    F = gate.shape[2]
    bf, f4 = jnp.bfloat16, jnp.float32
    dma = pltpu.SemaphoreType.DMA
    vm = pl.BlockSpec(memory_space=pltpu.VMEM)
    hb = pl.BlockSpec(memory_space=pl.ANY)
    return pl.pallas_call(
        functools.partial(moe_kernel, (Z, X, S, H, R, nc, top)),
        out_shape=jax.ShapeDtypeStruct((S, H), bf),
        in_specs=[vm, vm, vm, hb, hb, hb],
        out_specs=vm,
        scratch_shapes=[
            pltpu.VMEM((Z, nc, S, W), bf),
            pltpu.VMEM((Z, 16, LANES), f4),
            pltpu.VMEM((X, Z, LANES), f4),
            pltpu.VMEM((X, Z, LANES), f4),
            pltpu.VMEM((Z, X * R, LANES), bf),
            pltpu.VMEM((Z, LANES, X * R), bf),
            pltpu.VMEM((Z, nc, X * R, W), bf),
            pltpu.VMEM((Z, 2, nc, X * R, W), bf),
            pltpu.VMEM((D, 2 * F), bf),
            pltpu.VMEM((F, D), bf),
            pltpu.VMEM((Z, 2, nc, X * R, W), bf),
            pltpu.VMEM((Z, nc, X * R, W), bf),
            pltpu.VMEM((Z, nc, X * R, W), bf),
            pltpu.VMEM((Z, nc, X * R, W), bf),
            pltpu.VMEM((Z + 1, nc, S, W), bf),
            pltpu.VMEM((Z, nc, S, W), bf),
            dma((3,)),
            dma((Z,)),
            dma((Z,)),
            dma((2, Z // 2, nc)),
            dma((Z, nc)),
            dma((Z,)),
            dma((Z,)),
            dma((Z,)),
            dma((Z,)),
            dma((Z,)),
            dma((Z,)),
            dma((Z,)),
            dma((Z,)),
            dma((Z, nc)),
            dma((Z + 1, nc)),
        ],
        compiler_params=pltpu.CompilerParams(
            collective_id=0, has_side_effects=True, vmem_limit_bytes=48 * 1024 * 1024
        ),
        name="moe",
    )(tokens, base, table, gate, up, down)


def copy_for_each(value, axis):
    peers = lax.axis_size(axis)
    return lax.all_to_all(
        jnp.broadcast_to(value[None], (peers, *value.shape)), axis, 0, 0, tiled=True
    )


def of_everyone(value, axis):
    return copy_for_each(value, axis).astype(jnp.float32).sum(axis=0)


def in_blocks(value, dim, peers):
    before, after = (value.shape[:dim], value.shape[dim + 1 :])
    return jnp.moveaxis(value.reshape(*before, peers, -1, *after), dim, 0)


def summed_on_arrival(value, axis, dim):
    tiles = in_blocks(value, dim, lax.axis_size(axis))
    arrived = lax.all_to_all(tiles, axis, split_axis=0, concat_axis=0, tiled=True)
    return arrived.astype(jnp.float32).sum(axis=0)


def root_scale(activations, scale_gain):
    values = activations.astype(jnp.float32)
    factor = lax.rsqrt(jnp.mean(values * values, axis=-1, keepdims=True) + norm_eps)
    return (values * factor * scale_gain).astype(jnp.bfloat16)


def state_update(
    drive_rows, prior_state, decay_rate, frequency, log_step, input_map, output_map, skip_gain
):
    sequences = drive_rows.shape[0]
    groups = decay_rate.shape[0]
    driven = drive_rows.astype(jnp.float32).reshape(sequences, groups, -1)
    step_size = jnp.exp(log_step)[:, None]
    real_rate = -decay_rate
    magnitude = jnp.exp(real_rate * step_size)
    turn_real = magnitude * jnp.cos(frequency * step_size)
    turn_imag = magnitude * jnp.sin(frequency * step_size)
    denominator = real_rate * real_rate + frequency * frequency
    hold_real = ((turn_real - 1.0) * real_rate + turn_imag * frequency) / denominator
    hold_imag = (turn_imag * real_rate - (turn_real - 1.0) * frequency) / denominator
    push_real = jnp.einsum("sgh,gph->sgp", driven, input_map[0])
    push_imag = jnp.einsum("sgh,gph->sgp", driven, input_map[1])
    enter_real = push_real * hold_real - push_imag * hold_imag
    enter_imag = push_real * hold_imag + push_imag * hold_real
    old_real = prior_state[0].reshape(sequences, groups, -1)
    old_imag = prior_state[1].reshape(sequences, groups, -1)
    fresh_real = turn_real * old_real - turn_imag * old_imag + enter_real
    fresh_imag = turn_real * old_imag + turn_imag * old_real + enter_imag
    readout = jnp.einsum("ghp,sgp->sgh", output_map[0], fresh_real)
    readout = readout - jnp.einsum("ghp,sgp->sgh", output_map[1], fresh_imag)
    readout = readout.reshape(sequences, -1) + skip_gain * drive_rows.astype(jnp.float32)
    fresh = jnp.stack([fresh_real.reshape(sequences, -1), fresh_imag.reshape(sequences, -1)])
    return (readout, fresh)


def body(
    tokens,
    prior_state,
    mix_gain,
    in_weight,
    decay_rate,
    frequency,
    log_step,
    input_map,
    output_map,
    skip_gain,
    out_weight,
    channel_gain,
    expert_gate,
    expert_up,
    expert_down,
    shared_gate,
    shared_up,
    shared_down,
    routes,
    route_weights,
):
    normed = root_scale(tokens, mix_gain)
    drive_rows = jnp.dot(normed, in_weight, preferred_element_type=jnp.float32).astype(jnp.bfloat16)
    readout, new_state = state_update(
        drive_rows, prior_state, decay_rate, frequency, log_step, input_map, output_map, skip_gain
    )
    activated = jax.nn.gelu(readout).astype(jnp.bfloat16)
    partial_value = jnp.dot(activated, out_weight, preferred_element_type=jnp.float32)
    mixer_out = of_everyone(partial_value.astype(jnp.bfloat16), "tp").astype(jnp.float32)
    middle = (tokens.astype(jnp.float32) + mixer_out).astype(jnp.bfloat16)
    second_normed = root_scale(middle, channel_gain)
    shared_gval = jnp.dot(second_normed, shared_gate, preferred_element_type=jnp.float32)
    shared_uval = jnp.dot(second_normed, shared_up, preferred_element_type=jnp.float32)
    shared_hidden = (jax.nn.silu(shared_gval) * shared_uval).astype(jnp.bfloat16)
    shared_piece = jnp.dot(shared_hidden, shared_down, preferred_element_type=jnp.float32)
    shared_out = summed_on_arrival(shared_piece.astype(jnp.bfloat16), "tp", 1)
    half_cols = middle.shape[1] // lax.axis_size("tp")
    own_middle = lax.dynamic_slice_in_dim(middle, lax.axis_index("tp") * half_cols, half_cols, 1)
    base = own_middle.astype(jnp.float32) + shared_out
    seq_rows, top_count = routes.shape
    pad = ((0, 8 - top_count), (0, LANES - seq_rows))
    table = jnp.concatenate(
        [
            jnp.pad(routes.T.astype(jnp.float32), pad, constant_values=-1.0),
            jnp.pad(route_weights.T, pad),
        ],
        axis=0,
    )
    layer_out = moe(second_normed, base, table, expert_gate, expert_up, expert_down, top_count)
    return (layer_out, new_state)


def solution(mesh):
    in_specs = (
        P(("grp", "ep"), None),
        P(None, ("grp", "ep"), "tp"),
        P(),
        P(None, "tp"),
        P("tp", None),
        P("tp", None),
        P("tp"),
        P(None, "tp", None, None),
        P(None, "tp", None, None),
        P("tp"),
        P("tp", None),
        P(),
        P("ep", None, "tp"),
        P("ep", None, "tp"),
        P("ep", "tp", None),
        P(None, "tp"),
        P(None, "tp"),
        P("tp", None),
        P(("grp", "ep"), None),
        P(("grp", "ep"), None),
    )
    out_specs = (P(("grp", "ep"), "tp"), P(None, ("grp", "ep"), "tp"))
    return jax.shard_map(body, mesh=mesh, in_specs=in_specs, out_specs=out_specs, check_vma=False)
```

```python
import functools

import jax
import jax.numpy as jnp
from jax import lax
from jax.experimental import pallas as pl
from jax.experimental.pallas import tpu as pltpu
from jax.sharding import PartitionSpec as P

MESH = pl.DeviceIdType.MESH
norm_eps = 1e-06
ROW_RING = 4
CHUNKS = 4
LANES = 128


def layer_kernel(
    cfg,
    active_ref,
    tokens_ref,
    gain_ref,
    table_ref,
    project_hbm,
    sgate_hbm,
    sup_hbm,
    sdown_hbm,
    gate_hbm,
    up_hbm,
    down_hbm,
    out_ref,
    project,
    mixed,
    mixed_in,
    middle,
    normed,
    s_in,
    s_out,
    s_hidden,
    s_part,
    s_part_in,
    gathered,
    tables,
    pick,
    spread,
    staged,
    rows_in,
    w_in,
    w_out,
    partial,
    partner_part,
    total,
    back,
    sums_in,
    sums_out,
    w_sem,
    m_sem,
    s_sem,
    t_send,
    t_recv,
    z_send,
    z_recv,
    x_send,
    x_recv,
    c_send,
    c_recv,
    p_send,
    p_recv,
    b_send,
    b_recv,
    r_send,
    r_recv,
):
    Z, X, S, H, R, nc, top = cfg
    W = H // nc
    half = Z // 2
    F = gate_hbm.shape[2]
    SF = sgate_hbm.shape[1]
    ep = lax.axis_index("ep")
    tp = lax.axis_index("tp")
    other = 1 - tp
    z, x = ep // X, lax.rem(ep, X)

    def at_z(offset):
        return {"ep": lax.rem(z + offset + Z, Z) * X + x}

    def at_x(offset):
        return {"ep": z * X + lax.rem(x + offset + X, X)}

    partner = {"tp": other}

    def send(src, dst, s_sem, r_sem, device):
        return pltpu.make_async_remote_copy(
            src_ref=src, dst_ref=dst, send_sem=s_sem, recv_sem=r_sem,
            device_id=device, device_id_type=MESH,
        )

    def project_copy():
        return pltpu.make_async_copy(project_hbm, project, w_sem.at[0])

    def shared_copies():
        return (
            pltpu.make_async_copy(sgate_hbm, s_in.at[:, pl.ds(0, SF)], w_sem.at[1]),
            pltpu.make_async_copy(sup_hbm, s_in.at[:, pl.ds(SF, SF)], w_sem.at[2]),
            pltpu.make_async_copy(sdown_hbm, s_out, w_sem.at[3]),
        )

    def expert_copies():
        return (
            pltpu.make_async_copy(gate_hbm.at[0], w_in.at[:, pl.ds(0, F)], w_sem.at[4]),
            pltpu.make_async_copy(up_hbm.at[0], w_in.at[:, pl.ds(F, F)], w_sem.at[5]),
            pltpu.make_async_copy(down_hbm.at[0], w_out, w_sem.at[6]),
        )

    project_copy().start()

    barrier = pltpu.get_barrier_semaphore()
    for device in (at_z(1), at_z(-1), *[at_x(d) for d in range(1, X)], partner):
        pl.semaphore_signal(barrier, inc=1, device_id=device, device_id_type=MESH)

    tables[0] = table_ref[...]
    project_copy().wait()
    for copy in (*shared_copies(), *expert_copies()):
        copy.start()
    active = active_ref[...]
    for h in range(2 * nc):
        cols = slice(h * W, (h + 1) * W)
        mixed[:, cols] = jnp.dot(active, project[:, cols], preferred_element_type=jnp.float32).astype(jnp.bfloat16)

    pl.semaphore_wait(barrier, X + 2)

    mixed_copy = send(mixed, mixed_in, m_sem.at[0], m_sem.at[1], partner)
    mixed_copy.start()

    def t_copy(way, k):
        if way == 0:
            return send(tables.at[k], tables.at[k + 1], t_send.at[0, k], t_recv.at[k + 1], at_z(1))
        r = lax.rem(Z - k, Z)
        return send(tables.at[r], tables.at[Z - k - 1], t_send.at[1, k], t_recv.at[Z - k - 1], at_z(-1))

    def t_stage(k):
        for way in (0, 1):
            limit = half - way

            @pl.when((k >= 1) & (k <= limit))
            def _():
                t_copy(way, k - 1).wait_recv()

            @pl.when(k + 1 <= limit)
            def _():
                t_copy(way, k).start()

    def z_copy(way, k, c):
        if way == 0:
            return send(gathered.at[k, c], gathered.at[k + 1, c], z_send.at[0, k, c], z_recv.at[k + 1, c], at_z(1))
        r = lax.rem(Z - k, Z)
        return send(gathered.at[r, c], gathered.at[Z - k - 1, c], z_send.at[1, k, c], z_recv.at[Z - k - 1, c], at_z(-1))

    def z_limit(way, c):
        mine = (c < nc // 2) if way == 0 else (c >= nc // 2)
        return half if mine else half - 1

    def z_stage(k, c):
        for way in (0, 1):
            limit = z_limit(way, c)

            @pl.when((k >= 1) & (k <= limit))
            def _():
                z_copy(way, k - 1, c).wait_recv()

            @pl.when(k + 1 <= limit)
            def _():
                z_copy(way, k, c).start()

    before = (
        lax.broadcasted_iota(jnp.int32, (LANES, LANES), 0) < lax.broadcasted_iota(jnp.int32, (LANES, LANES), 1)
    ).astype(jnp.float32).astype(jnp.bfloat16)
    offset = lax.broadcasted_iota(jnp.int32, (8, LANES), 0)
    column = offset + x
    column = jnp.where(column >= X, column - X, column)
    expert_of = jnp.where(offset < X, z * X + column, -2).astype(jnp.float32)

    def build(r):
        table = tables[r].astype(jnp.float32)
        named = jnp.zeros((8, LANES), jnp.float32)
        weight = jnp.zeros((8, LANES), jnp.float32)
        for k in range(top):
            hit = table[k : k + 1, :] == expert_of
            named = named + jnp.where(hit, 1.0, 0.0)
            weight = weight + jnp.where(hit, table[8 + k : 9 + k, :], 0.0)
        rank = jnp.dot(named.astype(jnp.bfloat16), before, preferred_element_type=jnp.float32)
        code = jnp.where(named > 0.0, rank, -1.0)
        slot = lax.broadcasted_iota(jnp.int32, (R, LANES), 0).astype(jnp.float32)
        parts, weighted = [], []
        for d in range(X):
            block = jnp.where(code[d : d + 1, :] == slot, 1.0, 0.0)
            parts.append(block)
            weighted.append(block * weight[d : d + 1, :])
        pick[r] = jnp.concatenate(parts, axis=0).astype(jnp.bfloat16)
        spread[r] = jnp.concatenate(weighted, axis=0).T.astype(jnp.bfloat16)

    t_stage(jnp.int32(0))
    build(0)

    mixed_copy.wait_recv()
    both = mixed[...].astype(jnp.float32) + mixed_in[...].astype(jnp.float32)
    middle[...] = (tokens_ref[...].astype(jnp.float32) + both).astype(jnp.bfloat16)
    values = middle[...].astype(jnp.float32)
    factor = lax.rsqrt(jnp.mean(values * values, axis=-1, keepdims=True) + norm_eps)
    normed[...] = (values * factor * gain_ref[...]).astype(jnp.bfloat16)

    def own(c):
        return pl.ds(pl.multiple_of(tp * H + c * W, W), W)

    for c in range(nc):
        gathered[0, c] = normed[:, own(c)]
        z_stage(jnp.int32(0), c)

    def shared_hidden():
        for copy in shared_copies():
            copy.wait()
        acc = jnp.dot(normed[...], s_in[...], preferred_element_type=jnp.float32)
        s_hidden[...] = (jax.nn.silu(acc[:, :SF]) * acc[:, SF:]).astype(jnp.bfloat16)

    s_copy = send(s_part.at[other], s_part_in, s_sem.at[0], s_sem.at[1], partner)

    def shared_partial():
        for h in range(2):
            for c in range(nc):
                s_part[h, :, pl.ds(c * W, W)] = jnp.dot(
                    s_hidden[...], s_out[:, pl.ds(h * H + c * W, W)], preferred_element_type=jnp.float32
                ).astype(jnp.bfloat16)
        s_copy.start()

    def x_copy(r, d):
        rows = pl.ds(d * R, R)
        return send(staged.at[r, :, rows, :], rows_in.at[r, tp, :, rows, :], x_send.at[r], x_recv.at[r], at_x(d))

    def c_copy(r):
        return send(rows_in.at[r, tp], rows_in.at[r, tp], c_send.at[r], c_recv.at[r], partner)

    def p_copy(r):
        return send(partial.at[r, other], partner_part.at[r], p_send.at[r], p_recv.at[r], partner)

    def b_copy(r, d):
        rows = pl.ds(d * R, R)
        return send(total.at[r, :, rows, :], back.at[r, :, rows, :], b_send.at[r], b_recv.at[r], at_x(-d))

    def select(r):
        for c in range(nc):
            chosen = jnp.dot(
                pick[r, :, pl.ds(0, S)], gathered[r, c], preferred_element_type=jnp.float32
            ).astype(jnp.bfloat16)
            rows_in[r, tp, c, pl.ds(0, R), :] = chosen[:R]
            staged[r, c] = chosen
        for d in range(1, X):
            x_copy(r, d).start()

    rest = pl.ds(R, (X - 1) * R)

    def hand_over(r):
        send(staged.at[r, :, rest, :], rows_in.at[r, tp, :, rest, :], x_send.at[r], x_recv.at[r], at_x(1)).wait_recv()
        c_copy(r).start()

    def expert(r):
        send(rows_in.at[r, other], rows_in.at[r, other], c_send.at[r], c_recv.at[r], partner).wait_recv()
        acc = jnp.zeros((X * R, 2 * F), jnp.float32)
        for h in range(2):
            for c in range(nc):
                acc = acc + jnp.dot(
                    rows_in[r, h, c], w_in[pl.ds(h * H + c * W, W), :], preferred_element_type=jnp.float32
                )
        hidden = (jax.nn.silu(acc[:, :F]) * acc[:, F:]).astype(jnp.bfloat16)
        for h in range(2):
            for c in range(nc):
                partial[r, h, c] = jnp.dot(
                    hidden, w_out[:, pl.ds(h * H + c * W, W)], preferred_element_type=jnp.float32
                ).astype(jnp.bfloat16)
        p_copy(r).start()

    def join(r):
        p_copy(r).wait_recv()
        for c in range(nc):
            y = (partial[r, tp, c].astype(jnp.float32) + partner_part[r, c].astype(jnp.float32)).astype(jnp.bfloat16)
            back[r, c, pl.ds(0, R), :] = y[:R]
            total[r, c] = y
        for d in range(1, X):
            b_copy(r, d).start()

    def of_pair(stage, k, way, least=0):
        if way == 0:
            @pl.when((k >= least) & (k <= half))
            def _():
                stage(k)
        else:
            @pl.when((k >= 1) & (k < half))
            def _():
                stage(Z - k)

    def step(i, carry):
        @pl.when(i <= half)
        def _():
            t_stage(i)

        z_stage(i, 0)
        of_pair(build, i, 0, 1)
        of_pair(build, i, 1, 1)
        of_pair(select, i - 1, 0)
        of_pair(select, i - 1, 1)
        z_stage(i, 1)

        @pl.when(i == 1)
        def _():
            shared_hidden()

        @pl.when(i == 2)
        def _():
            shared_partial()

        @pl.when(i == 3)
        def _():
            for copy in expert_copies():
                copy.wait()

        of_pair(hand_over, i - 2, 0)
        of_pair(hand_over, i - 2, 1)
        of_pair(expert, i - 3, 0)
        z_stage(i, 2)
        of_pair(expert, i - 3, 1)
        of_pair(join, i - 4, 0)
        z_stage(i, 3)
        of_pair(join, i - 4, 1)
        return carry

    lax.fori_loop(1, half + 5, step, 0)

    def r_copy(way, k, c):
        if way == 0:
            return send(sums_out.at[k, c], sums_in.at[k - 1, c], r_send.at[k, c], r_recv.at[k - 1, c], at_z(-1))
        return send(sums_out.at[Z - k, c], sums_in.at[Z - k + 1, c], r_send.at[Z - k, c], r_recv.at[Z - k + 1, c], at_z(1))

    def share_of(r, c):
        return jnp.dot(spread[r, pl.ds(0, S), :], back[r, c], preferred_element_type=jnp.float32)

    def back_wait(r):
        send(total.at[r, :, rest, :], back.at[r, :, rest, :], b_send.at[r], b_recv.at[r], at_x(1)).wait_recv()

    def go_back(i, carry):
        k = half - i
        back_wait(k)

        @pl.when(k < half)
        def _():
            back_wait(Z - k)

        for c in range(nc):
            for way in (0, 1):
                limit = z_limit(way, c)
                r = k if way == 0 else Z - k

                @pl.when(k <= limit)
                def _():
                    mine = share_of(r, c)

                    @pl.when(k == limit)
                    def _():
                        sums_out[r, c] = mine.astype(jnp.bfloat16)

                    @pl.when(k < limit)
                    def _():
                        r_copy(way, k + 1, c).wait_recv()
                        sums_out[r, c] = (mine + sums_in[r, c].astype(jnp.float32)).astype(jnp.bfloat16)

                    r_copy(way, k, c).start()
        return carry

    lax.fori_loop(0, half, go_back, 0)

    back_wait(0)
    s_copy.wait_recv()
    for c in range(nc):
        mine = share_of(0, c) + middle[:, own(c)].astype(jnp.float32)
        mine = mine + s_part[tp, :, pl.ds(c * W, W)].astype(jnp.float32)
        mine = mine + s_part_in[:, pl.ds(c * W, W)].astype(jnp.float32)
        r_copy(0, 1, c).wait_recv()
        r_copy(1, 1, c).wait_recv()
        mine = mine + sums_in[0, c].astype(jnp.float32) + sums_in[Z, c].astype(jnp.float32)
        out_ref[:, pl.ds(c * W, W)] = mine.astype(out_ref.dtype)

    mixed_copy.wait_send()
    s_copy.wait_send()

    def drain(k, carry):
        for way in (0, 1):
            @pl.when(k + 1 <= half - way)
            def _():
                t_copy(way, k).wait_send()

        for c in range(nc):
            for way in (0, 1):
                limit = z_limit(way, c)

                @pl.when(k + 1 <= limit)
                def _():
                    z_copy(way, k, c).wait_send()
                    r_copy(way, k + 1, c).wait_send()
        return carry

    lax.fori_loop(0, half, drain, 0)

    def drain_rows(r, carry):
        send(staged.at[r, :, rest, :], rows_in.at[r, tp, :, rest, :], x_send.at[r], x_recv.at[r], at_x(1)).wait_send()
        c_copy(r).wait_send()
        p_copy(r).wait_send()
        send(total.at[r, :, rest, :], back.at[r, :, rest, :], b_send.at[r], b_recv.at[r], at_x(1)).wait_send()
        return carry

    lax.fori_loop(0, Z, drain_rows, 0)


def layer(active, tokens, gain, table, project, sgate, sup, sdown, gate, up, down, top):
    S, D = tokens.shape
    H = D // lax.axis_size("tp")
    X = ROW_RING
    Z = lax.axis_size("ep") // X
    nc = CHUNKS
    W = H // nc
    R = 16
    F = gate.shape[2]
    SF = sgate.shape[1]
    bf = jnp.bfloat16
    dma = pltpu.SemaphoreType.DMA
    vm = pl.BlockSpec(memory_space=pltpu.VMEM)
    hb = pl.BlockSpec(memory_space=pl.ANY)
    return pl.pallas_call(
        functools.partial(layer_kernel, (Z, X, S, H, R, nc, top)),
        out_shape=jax.ShapeDtypeStruct((S, H), bf),
        in_specs=[vm] * 4 + [hb] * 7,
        out_specs=vm,
        scratch_shapes=[
            pltpu.VMEM(project.shape, bf),
            pltpu.VMEM((S, D), bf),
            pltpu.VMEM((S, D), bf),
            pltpu.VMEM((S, D), bf),
            pltpu.VMEM((S, D), bf),
            pltpu.VMEM((D, 2 * SF), bf),
            pltpu.VMEM((SF, D), bf),
            pltpu.VMEM((S, SF), bf),
            pltpu.VMEM((2, S, H), bf),
            pltpu.VMEM((S, H), bf),
            pltpu.VMEM((Z, nc, S, W), bf),
            pltpu.VMEM((Z, 16, LANES), bf),
            pltpu.VMEM((Z, X * R, LANES), bf),
            pltpu.VMEM((Z, LANES, X * R), bf),
            pltpu.VMEM((Z, nc, X * R, W), bf),
            pltpu.VMEM((Z, 2, nc, X * R, W), bf),
            pltpu.VMEM((D, 2 * F), bf),
            pltpu.VMEM((F, D), bf),
            pltpu.VMEM((Z, 2, nc, X * R, W), bf),
            pltpu.VMEM((Z, nc, X * R, W), bf),
            pltpu.VMEM((Z, nc, X * R, W), bf),
            pltpu.VMEM((Z, nc, X * R, W), bf),
            pltpu.VMEM((Z + 1, nc, S, W), bf),
            pltpu.VMEM((Z, nc, S, W), bf),
            dma((7,)),
            dma((2,)),
            dma((2,)),
            dma((2, Z // 2)),
            dma((Z,)),
            dma((2, Z // 2, nc)),
            dma((Z, nc)),
            dma((Z,)),
            dma((Z,)),
            dma((Z,)),
            dma((Z,)),
            dma((Z,)),
            dma((Z,)),
            dma((Z,)),
            dma((Z,)),
            dma((Z, nc)),
            dma((Z + 1, nc)),
        ],
        compiler_params=pltpu.CompilerParams(
            collective_id=0, has_side_effects=True, vmem_limit_bytes=56 * 1024 * 1024
        ),
        name="layer",
    )(active, tokens, gain[None, :], table, project, sgate, sup, sdown, gate, up, down)


def mixer_kernel(
    tokens_ref,
    prior_hbm,
    gain_ref,
    weight_hbm,
    decay_ref,
    freq_ref,
    step_ref,
    imap_ref,
    omap_ref,
    skip_ref,
    active_ref,
    state_hbm,
    weight,
    old,
    fresh,
    in_sem,
    out_sem,
):
    S, D = tokens_ref.shape
    width = weight.shape[1]
    groups, entries = decay_ref.shape
    members = width // groups
    f4, bf = jnp.float32, jnp.bfloat16
    lane_groups = LANES // entries
    block = LANES // members
    cols = block * entries

    def weight_copy():
        return pltpu.make_async_copy(weight_hbm, weight, in_sem.at[0])

    def old_copy(part):
        return pltpu.make_async_copy(prior_hbm.at[part], old.at[part], in_sem.at[1 + part])

    def state_copy(part, q):
        lanes = pl.ds(q * cols, cols)
        return pltpu.make_async_copy(fresh.at[part, :, lanes], state_hbm.at[part, :, lanes], out_sem.at[part, q])

    weight_copy().start()
    old_copy(0).start()
    old_copy(1).start()

    eye = lax.broadcasted_iota(jnp.int32, (groups, groups), 0) == lax.broadcasted_iota(jnp.int32, (groups, groups), 1)
    log_column = jnp.sum(jnp.where(eye, step_ref[...], 0.0), axis=1, keepdims=True)
    step_size = jnp.exp(log_column)
    real_rate = -decay_ref[...]
    frequency = freq_ref[...]
    magnitude = jnp.exp(real_rate * step_size)
    turn_real = magnitude * jnp.cos(frequency * step_size)
    turn_imag = magnitude * jnp.sin(frequency * step_size)
    denominator = real_rate * real_rate + frequency * frequency
    hold_real = ((turn_real - 1.0) * real_rate + turn_imag * frequency) / denominator
    hold_imag = (turn_imag * real_rate - (turn_real - 1.0) * frequency) / denominator
    doubled = [jnp.concatenate([v] * lane_groups, axis=1) for v in (turn_real, turn_imag, hold_real, hold_imag)]
    row_group = lax.broadcasted_iota(jnp.int32, (groups, LANES), 0)
    lane_group = lax.broadcasted_iota(jnp.int32, (groups, LANES), 1) // entries

    values = tokens_ref[...].astype(f4)
    factor = lax.rsqrt(jnp.mean(values * values, axis=-1, keepdims=True) + norm_eps)
    normed = (values * factor * gain_ref[...]).astype(bf)
    weight_copy().wait()
    drive = jnp.dot(normed, weight[...], preferred_element_type=f4).astype(bf)
    old_copy(0).wait()
    old_copy(1).wait()

    in_row = lax.broadcasted_iota(jnp.int32, (LANES, LANES), 0) // members
    in_lane = lax.broadcasted_iota(jnp.int32, (LANES, LANES), 1) // entries
    out_row = lax.broadcasted_iota(jnp.int32, (LANES, 2 * LANES), 0) // members
    out_lane = lax.broadcasted_iota(jnp.int32, (LANES, 2 * LANES), 1) // entries

    for q in range(width // LANES):
        channels = slice(q * LANES, (q + 1) * LANES)
        mine = drive[:, channels]
        maps = [jnp.concatenate([imap_ref[part, channels, :]] * lane_groups, axis=1) for part in range(2)]
        outs = [jnp.concatenate([omap_ref[part, channels, :]] * (2 * lane_groups), axis=1) for part in range(2)]
        readout = mine.astype(f4) * skip_ref[:, channels]
        for m in range(cols // LANES):
            mask = in_row == in_lane + m * lane_groups
            both = jnp.concatenate([jnp.where(mask, v, 0.0) for v in maps], axis=1).astype(bf)
            push = jnp.dot(mine, both, preferred_element_type=f4)
            push_real, push_imag = push[:, :LANES], push[:, LANES:]
            first = q * block + m * lane_groups
            tr, ti, hr, hi = [
                jnp.sum(jnp.where(row_group == lane_group + first, v, 0.0), axis=0, keepdims=True) for v in doubled
            ]
            at = slice(q * cols + m * LANES, q * cols + (m + 1) * LANES)
            old_real, old_imag = old[0, :, at], old[1, :, at]
            fresh[0, :, at] = tr * old_real - ti * old_imag + (push_real * hr - push_imag * hi)
            fresh[1, :, at] = tr * old_imag + ti * old_real + (push_real * hi + push_imag * hr)
        state_copy(0, q).start()
        state_copy(1, q).start()
        for h in range(cols // (2 * LANES)):
            at = slice(q * cols + h * 2 * LANES, q * cols + (h + 1) * 2 * LANES)
            mask = out_row == out_lane + h * 2 * lane_groups
            for part in range(2):
                spread_out = jnp.where(mask, outs[part] if part == 0 else -outs[part], 0.0).astype(bf)
                readout = readout + lax.dot_general(
                    fresh[part, :, at].astype(bf), spread_out, (((1,), (1,)), ((), ())), preferred_element_type=f4
                )
        active_ref[:, channels] = jax.nn.gelu(readout).astype(bf)
    for q in range(width // LANES):
        for part in range(2):
            state_copy(part, q).wait()


def mixer(tokens, prior, gain, weight, decay, freq, log_step, imap, omap, skip):
    S, D = tokens.shape
    width = weight.shape[1]
    vm = pl.BlockSpec(memory_space=pltpu.VMEM)
    hb = pl.BlockSpec(memory_space=pl.ANY)
    dma = pltpu.SemaphoreType.DMA
    by_channel = (2, width, imap.shape[2])
    return pl.pallas_call(
        mixer_kernel,
        out_shape=(
            jax.ShapeDtypeStruct((S, width), jnp.bfloat16),
            jax.ShapeDtypeStruct(prior.shape, jnp.float32),
        ),
        in_specs=[vm, hb, vm, hb, vm, vm, vm, vm, vm, vm],
        out_specs=(vm, hb),
        scratch_shapes=[
            pltpu.VMEM(weight.shape, weight.dtype),
            pltpu.VMEM(prior.shape, jnp.float32),
            pltpu.VMEM(prior.shape, jnp.float32),
            dma((3,)),
            dma((2, width // LANES)),
        ],
        compiler_params=pltpu.CompilerParams(vmem_limit_bytes=32 * 1024 * 1024),
        name="mixer",
    )(
        tokens,
        prior,
        gain[None, :],
        weight,
        decay,
        freq,
        log_step[None, :],
        jnp.swapaxes(imap, 2, 3).reshape(by_channel),
        omap.reshape(by_channel),
        skip[None, :],
    )


def body(
    tokens,
    prior_state,
    mix_gain,
    in_weight,
    decay_rate,
    frequency,
    log_step,
    input_map,
    output_map,
    skip_gain,
    out_weight,
    channel_gain,
    expert_gate,
    expert_up,
    expert_down,
    shared_gate,
    shared_up,
    shared_down,
    routes,
    route_weights,
):
    activated, new_state = mixer(
        tokens, prior_state, mix_gain, in_weight, decay_rate, frequency, log_step, input_map, output_map, skip_gain
    )
    seq_rows, top_count = routes.shape
    pad = ((0, 8 - top_count), (0, LANES - seq_rows))
    table = jnp.concatenate(
        [
            jnp.pad(routes.T.astype(jnp.float32), pad, constant_values=-1.0),
            jnp.pad(route_weights.T, pad),
        ],
        axis=0,
    ).astype(jnp.bfloat16)
    layer_out = layer(
        activated,
        tokens,
        channel_gain,
        table,
        out_weight,
        shared_gate,
        shared_up,
        shared_down,
        expert_gate,
        expert_up,
        expert_down,
        top_count,
    )
    return (layer_out, new_state)


def solution(mesh):
    in_specs = (
        P(("grp", "ep"), None),
        P(None, ("grp", "ep"), "tp"),
        P(),
        P(None, "tp"),
        P("tp", None),
        P("tp", None),
        P("tp"),
        P(None, "tp", None, None),
        P(None, "tp", None, None),
        P("tp"),
        P("tp", None),
        P(),
        P("ep", None, "tp"),
        P("ep", None, "tp"),
        P("ep", "tp", None),
        P(None, "tp"),
        P(None, "tp"),
        P("tp", None),
        P(("grp", "ep"), None),
        P(("grp", "ep"), None),
    )
    out_specs = (P(("grp", "ep"), "tp"), P(None, ("grp", "ep"), "tp"))
    return jax.shard_map(body, mesh=mesh, in_specs=in_specs, out_specs=out_specs, check_vma=False)
```

```python
import functools

import jax
import jax.numpy as jnp
from jax import lax
from jax.experimental import pallas as pl
from jax.experimental.pallas import tpu as pltpu
from jax.sharding import PartitionSpec as P

MESH = pl.DeviceIdType.MESH
norm_eps = 1e-06
ROW_RING = 4
CHUNKS = 4
LANES = 128
VMEM_ALL = 63 * 1024 * 1024


def layer_kernel(
    cfg,
    mixed_hbm,
    tokens_hbm,
    gain_hbm,
    routes_hbm,
    shares_hbm,
    sgate_hbm,
    sup_hbm,
    sdown_hbm,
    gate_hbm,
    up_hbm,
    down_hbm,
    out_ref,
    tokens_ref,
    gain_ref,
    routes_ref,
    shares_ref,
    table,
    mixed,
    mixed_in,
    middle,
    normed,
    s_in,
    s_out,
    s_hidden,
    s_part,
    s_part_in,
    gathered,
    tables,
    pick,
    spread,
    staged,
    rows_in,
    w_in,
    w_out,
    partial,
    partner_part,
    total,
    back,
    sums_in,
    sums_out,
    w_sem,
    m_sem,
    s_sem,
    t_send,
    t_recv,
    z_send,
    z_recv,
    x_send,
    x_recv,
    c_send,
    c_recv,
    p_send,
    p_recv,
    b_send,
    b_recv,
    r_send,
    r_recv,
):
    Z, X, S, H, R, nc, top = cfg
    W = H // nc
    half = Z // 2
    F = gate_hbm.shape[2]
    SF = sgate_hbm.shape[1]
    ep = lax.axis_index("ep")
    tp = lax.axis_index("tp")
    other = 1 - tp
    z, x = ep // X, lax.rem(ep, X)

    def at_z(offset):
        return {"ep": lax.rem(z + offset + Z, Z) * X + x}

    def at_x(offset):
        return {"ep": z * X + lax.rem(x + offset + X, X)}

    partner = {"tp": other}

    def send(src, dst, s_sem, r_sem, device):
        return pltpu.make_async_remote_copy(
            src_ref=src, dst_ref=dst, send_sem=s_sem, recv_sem=r_sem,
            device_id=device, device_id_type=MESH,
        )

    def shared_copies():
        return (
            pltpu.make_async_copy(sgate_hbm, s_in.at[:, pl.ds(0, SF)], w_sem.at[1]),
            pltpu.make_async_copy(sup_hbm, s_in.at[:, pl.ds(SF, SF)], w_sem.at[2]),
            pltpu.make_async_copy(sdown_hbm, s_out, w_sem.at[3]),
        )

    def expert_copies():
        return (
            pltpu.make_async_copy(gate_hbm.at[0], w_in.at[:, pl.ds(0, F)], w_sem.at[4]),
            pltpu.make_async_copy(up_hbm.at[0], w_in.at[:, pl.ds(F, F)], w_sem.at[5]),
            pltpu.make_async_copy(down_hbm.at[0], w_out, w_sem.at[6]),
        )

    small = [
        pltpu.make_async_copy(src, dst, w_sem.at[7 + i])
        for i, (src, dst) in enumerate(
            (
                (mixed_hbm, mixed),
                (routes_hbm, routes_ref),
                (shares_hbm, shares_ref),
                (tokens_hbm, tokens_ref),
                (gain_hbm, gain_ref),
            )
        )
    ]
    for copy in small:
        copy.start()

    barrier = pltpu.get_barrier_semaphore()
    for device in (at_z(1), at_z(-1), *[at_x(d) for d in range(1, X)], partner):
        pl.semaphore_signal(barrier, inc=1, device_id=device, device_id_type=MESH)

    table[...] = jnp.where(lax.broadcasted_iota(jnp.int32, (16, LANES), 0) < 8, -1.0, 0.0)
    for copy in small[:3]:
        copy.wait()
    table[pl.ds(0, top), pl.ds(0, S)] = routes_ref[...].astype(jnp.float32)
    table[pl.ds(8, top), pl.ds(0, S)] = shares_ref[...]
    tables[0] = table[...].astype(jnp.bfloat16)
    for copy in (*shared_copies(), *expert_copies()):
        copy.start()
    pl.semaphore_wait(barrier, X + 2)

    mixed_copy = send(mixed, mixed_in, m_sem.at[0], m_sem.at[1], partner)
    mixed_copy.start()

    def t_copy(way, k):
        if way == 0:
            return send(tables.at[k], tables.at[k + 1], t_send.at[0, k], t_recv.at[k + 1], at_z(1))
        r = lax.rem(Z - k, Z)
        return send(tables.at[r], tables.at[Z - k - 1], t_send.at[1, k], t_recv.at[Z - k - 1], at_z(-1))

    def t_stage(k):
        for way in (0, 1):
            limit = half - way

            @pl.when((k >= 1) & (k <= limit))
            def _():
                t_copy(way, k - 1).wait_recv()

            @pl.when(k + 1 <= limit)
            def _():
                t_copy(way, k).start()

    def z_copy(way, k, c):
        if way == 0:
            return send(gathered.at[k, c], gathered.at[k + 1, c], z_send.at[0, k, c], z_recv.at[k + 1, c], at_z(1))
        r = lax.rem(Z - k, Z)
        return send(gathered.at[r, c], gathered.at[Z - k - 1, c], z_send.at[1, k, c], z_recv.at[Z - k - 1, c], at_z(-1))

    def z_limit(way, c):
        mine = (c < nc // 2) if way == 0 else (c >= nc // 2)
        return half if mine else half - 1

    def z_stage(k, c):
        for way in (0, 1):
            limit = z_limit(way, c)

            @pl.when((k >= 1) & (k <= limit))
            def _():
                z_copy(way, k - 1, c).wait_recv()

            @pl.when(k + 1 <= limit)
            def _():
                z_copy(way, k, c).start()

    before = (
        lax.broadcasted_iota(jnp.int32, (LANES, LANES), 0) < lax.broadcasted_iota(jnp.int32, (LANES, LANES), 1)
    ).astype(jnp.float32).astype(jnp.bfloat16)
    offset = lax.broadcasted_iota(jnp.int32, (8, LANES), 0)
    column = offset + x
    column = jnp.where(column >= X, column - X, column)
    expert_of = jnp.where(offset < X, z * X + column, -2).astype(jnp.float32)

    def build(r):
        table = tables[r].astype(jnp.float32)
        named = jnp.zeros((8, LANES), jnp.float32)
        weight = jnp.zeros((8, LANES), jnp.float32)
        for k in range(top):
            hit = table[k : k + 1, :] == expert_of
            named = named + jnp.where(hit, 1.0, 0.0)
            weight = weight + jnp.where(hit, table[8 + k : 9 + k, :], 0.0)
        rank = jnp.dot(named.astype(jnp.bfloat16), before, preferred_element_type=jnp.float32)
        code = jnp.where(named > 0.0, rank, -1.0)
        slot = lax.broadcasted_iota(jnp.int32, (R, LANES), 0).astype(jnp.float32)
        parts, weighted = [], []
        for d in range(X):
            block = jnp.where(code[d : d + 1, :] == slot, 1.0, 0.0)
            parts.append(block)
            weighted.append(block * weight[d : d + 1, :])
        pick[r] = jnp.concatenate(parts, axis=0).astype(jnp.bfloat16)
        spread[r] = jnp.concatenate(weighted, axis=0).T.astype(jnp.bfloat16)

    t_stage(jnp.int32(0))
    build(0)

    for copy in small[3:]:
        copy.wait()
    mixed_copy.wait_recv()
    both = mixed[...].astype(jnp.float32) + mixed_in[...].astype(jnp.float32)
    middle[...] = (tokens_ref[...].astype(jnp.float32) + both).astype(jnp.bfloat16)
    values = middle[...].astype(jnp.float32)
    factor = lax.rsqrt(jnp.mean(values * values, axis=-1, keepdims=True) + norm_eps)
    normed[...] = (values * factor * gain_ref[...]).astype(jnp.bfloat16)

    def own(c):
        return pl.ds(pl.multiple_of(tp * H + c * W, W), W)

    for c in range(nc):
        gathered[0, c] = normed[:, own(c)]
        z_stage(jnp.int32(0), c)

    def shared_hidden():
        for copy in shared_copies():
            copy.wait()
        acc = jnp.dot(normed[...], s_in[...], preferred_element_type=jnp.float32)
        s_hidden[...] = (jax.nn.silu(acc[:, :SF]) * acc[:, SF:]).astype(jnp.bfloat16)

    s_copy = send(s_part.at[other], s_part_in, s_sem.at[0], s_sem.at[1], partner)

    def shared_partial():
        for h in range(2):
            for c in range(nc):
                s_part[h, :, pl.ds(c * W, W)] = jnp.dot(
                    s_hidden[...], s_out[:, pl.ds(h * H + c * W, W)], preferred_element_type=jnp.float32
                ).astype(jnp.bfloat16)
        s_copy.start()

    def x_copy(r, d):
        rows = pl.ds(d * R, R)
        return send(staged.at[r, :, rows, :], rows_in.at[r, tp, :, rows, :], x_send.at[r], x_recv.at[r], at_x(d))

    def c_copy(r):
        return send(rows_in.at[r, tp], rows_in.at[r, tp], c_send.at[r], c_recv.at[r], partner)

    def p_copy(r):
        return send(partial.at[r, other], partner_part.at[r], p_send.at[r], p_recv.at[r], partner)

    def b_copy(r, d):
        rows = pl.ds(d * R, R)
        return send(total.at[r, :, rows, :], back.at[r, :, rows, :], b_send.at[r], b_recv.at[r], at_x(-d))

    def select(r):
        for c in range(nc):
            chosen = jnp.dot(
                pick[r, :, pl.ds(0, S)], gathered[r, c], preferred_element_type=jnp.float32
            ).astype(jnp.bfloat16)
            rows_in[r, tp, c, pl.ds(0, R), :] = chosen[:R]
            staged[r, c] = chosen
        for d in range(1, X):
            x_copy(r, d).start()

    rest = pl.ds(R, (X - 1) * R)

    def hand_over(r):
        send(staged.at[r, :, rest, :], rows_in.at[r, tp, :, rest, :], x_send.at[r], x_recv.at[r], at_x(1)).wait_recv()
        c_copy(r).start()

    def expert(r):
        send(rows_in.at[r, other], rows_in.at[r, other], c_send.at[r], c_recv.at[r], partner).wait_recv()
        acc = jnp.zeros((X * R, 2 * F), jnp.float32)
        for h in range(2):
            for c in range(nc):
                acc = acc + jnp.dot(
                    rows_in[r, h, c], w_in[pl.ds(h * H + c * W, W), :], preferred_element_type=jnp.float32
                )
        hidden = (jax.nn.silu(acc[:, :F]) * acc[:, F:]).astype(jnp.bfloat16)
        for h in range(2):
            for c in range(nc):
                partial[r, h, c] = jnp.dot(
                    hidden, w_out[:, pl.ds(h * H + c * W, W)], preferred_element_type=jnp.float32
                ).astype(jnp.bfloat16)
        p_copy(r).start()

    def join(r):
        p_copy(r).wait_recv()
        for c in range(nc):
            y = (partial[r, tp, c].astype(jnp.float32) + partner_part[r, c].astype(jnp.float32)).astype(jnp.bfloat16)
            back[r, c, pl.ds(0, R), :] = y[:R]
            total[r, c] = y

    def hand_back(r):
        for d in range(1, X):
            b_copy(r, d).start()

    def of_pair(stage, k, way, least=0):
        if way == 0:
            @pl.when((k >= least) & (k <= half))
            def _():
                stage(k)
        else:
            @pl.when((k >= 1) & (k < half))
            def _():
                stage(Z - k)

    def step(i, carry):
        @pl.when(i <= half)
        def _():
            t_stage(i)

        z_stage(i, 0)
        of_pair(build, i, 0, 1)
        of_pair(build, i, 1, 1)
        of_pair(select, i - 1, 0)
        of_pair(select, i - 1, 1)
        z_stage(i, 1)

        @pl.when(i == 1)
        def _():
            shared_hidden()

        @pl.when(i == 2)
        def _():
            shared_partial()

        @pl.when(i == 3)
        def _():
            for copy in expert_copies():
                copy.wait()

        of_pair(hand_over, i - 2, 0)
        of_pair(hand_over, i - 2, 1)
        of_pair(expert, i - 3, 0)
        z_stage(i, 2)
        of_pair(expert, i - 3, 1)
        of_pair(join, i - 4, 0)
        z_stage(i, 3)
        of_pair(join, i - 4, 1)

        @pl.when(i - 4 >= half - 1)
        def _():
            of_pair(hand_back, i - 4, 0)
            of_pair(hand_back, i - 4, 1)

        return carry

    lax.fori_loop(1, half + 5, step, 0)

    def r_copy(way, k, c):
        if way == 0:
            return send(sums_out.at[k, c], sums_in.at[k - 1, c], r_send.at[k, c], r_recv.at[k - 1, c], at_z(-1))
        return send(sums_out.at[Z - k, c], sums_in.at[Z - k + 1, c], r_send.at[Z - k, c], r_recv.at[Z - k + 1, c], at_z(1))

    def share_of(r, c):
        return jnp.dot(spread[r, pl.ds(0, S), :], back[r, c], preferred_element_type=jnp.float32)

    def back_wait(r):
        send(total.at[r, :, rest, :], back.at[r, :, rest, :], b_send.at[r], b_recv.at[r], at_x(1)).wait_recv()

    def go_back(i, carry):
        k = half - i
        of_pair(hand_back, k - 2, 0)
        of_pair(hand_back, k - 2, 1)
        back_wait(k)

        @pl.when(k < half)
        def _():
            back_wait(Z - k)

        for c in range(nc):
            for way in (0, 1):
                limit = z_limit(way, c)
                r = k if way == 0 else Z - k

                @pl.when(k <= limit)
                def _():
                    mine = share_of(r, c)

                    @pl.when(k == limit)
                    def _():
                        sums_out[r, c] = mine.astype(jnp.bfloat16)

                    @pl.when(k < limit)
                    def _():
                        r_copy(way, k + 1, c).wait_recv()
                        sums_out[r, c] = (mine + sums_in[r, c].astype(jnp.float32)).astype(jnp.bfloat16)

                    r_copy(way, k, c).start()
        return carry

    lax.fori_loop(0, half, go_back, 0)

    back_wait(0)
    s_copy.wait_recv()
    for c in range(nc):
        mine = share_of(0, c) + middle[:, own(c)].astype(jnp.float32)
        mine = mine + s_part[tp, :, pl.ds(c * W, W)].astype(jnp.float32)
        mine = mine + s_part_in[:, pl.ds(c * W, W)].astype(jnp.float32)
        r_copy(0, 1, c).wait_recv()
        r_copy(1, 1, c).wait_recv()
        mine = mine + sums_in[0, c].astype(jnp.float32) + sums_in[Z, c].astype(jnp.float32)
        out_ref[:, pl.ds(c * W, W)] = mine.astype(out_ref.dtype)

    mixed_copy.wait_send()
    s_copy.wait_send()

    def drain(k, carry):
        for way in (0, 1):
            @pl.when(k + 1 <= half - way)
            def _():
                t_copy(way, k).wait_send()

        for c in range(nc):
            for way in (0, 1):
                limit = z_limit(way, c)

                @pl.when(k + 1 <= limit)
                def _():
                    z_copy(way, k, c).wait_send()
                    r_copy(way, k + 1, c).wait_send()
        return carry

    lax.fori_loop(0, half, drain, 0)

    def drain_rows(r, carry):
        send(staged.at[r, :, rest, :], rows_in.at[r, tp, :, rest, :], x_send.at[r], x_recv.at[r], at_x(1)).wait_send()
        c_copy(r).wait_send()
        p_copy(r).wait_send()
        send(total.at[r, :, rest, :], back.at[r, :, rest, :], b_send.at[r], b_recv.at[r], at_x(1)).wait_send()
        return carry

    lax.fori_loop(0, Z, drain_rows, 0)


def layer(mixed, tokens, gain, routes, shares, sgate, sup, sdown, gate, up, down):
    top = routes.shape[1]
    S, D = tokens.shape
    H = D // lax.axis_size("tp")
    X = ROW_RING
    Z = lax.axis_size("ep") // X
    nc = CHUNKS
    W = H // nc
    R = 16
    F = gate.shape[2]
    SF = sgate.shape[1]
    bf = jnp.bfloat16
    dma = pltpu.SemaphoreType.DMA
    vm = pl.BlockSpec(memory_space=pltpu.VMEM)
    hb = pl.BlockSpec(memory_space=pl.ANY)
    return pl.pallas_call(
        functools.partial(layer_kernel, (Z, X, S, H, R, nc, top)),
        out_shape=jax.ShapeDtypeStruct((S, H), bf),
        in_specs=[hb] * 11,
        out_specs=vm,
        scratch_shapes=[
            pltpu.VMEM((S, D), bf),
            pltpu.VMEM((1, D), jnp.float32),
            pltpu.VMEM((top, S), jnp.int32),
            pltpu.VMEM((top, S), jnp.float32),
            pltpu.VMEM((16, LANES), jnp.float32),
            pltpu.VMEM((S, D), bf),
            pltpu.VMEM((S, D), bf),
            pltpu.VMEM((S, D), bf),
            pltpu.VMEM((S, D), bf),
            pltpu.VMEM((D, 2 * SF), bf),
            pltpu.VMEM((SF, D), bf),
            pltpu.VMEM((S, SF), bf),
            pltpu.VMEM((2, S, H), bf),
            pltpu.VMEM((S, H), bf),
            pltpu.VMEM((Z, nc, S, W), bf),
            pltpu.VMEM((Z, 16, LANES), bf),
            pltpu.VMEM((Z, X * R, LANES), bf),
            pltpu.VMEM((Z, LANES, X * R), bf),
            pltpu.VMEM((Z, nc, X * R, W), bf),
            pltpu.VMEM((Z, 2, nc, X * R, W), bf),
            pltpu.VMEM((D, 2 * F), bf),
            pltpu.VMEM((F, D), bf),
            pltpu.VMEM((Z, 2, nc, X * R, W), bf),
            pltpu.VMEM((Z, nc, X * R, W), bf),
            pltpu.VMEM((Z, nc, X * R, W), bf),
            pltpu.VMEM((Z, nc, X * R, W), bf),
            pltpu.VMEM((Z + 1, nc, S, W), bf),
            pltpu.VMEM((Z, nc, S, W), bf),
            dma((12,)),
            dma((2,)),
            dma((2,)),
            dma((2, Z // 2)),
            dma((Z,)),
            dma((2, Z // 2, nc)),
            dma((Z, nc)),
            dma((Z,)),
            dma((Z,)),
            dma((Z,)),
            dma((Z,)),
            dma((Z,)),
            dma((Z,)),
            dma((Z,)),
            dma((Z,)),
            dma((Z, nc)),
            dma((Z + 1, nc)),
        ],
        compiler_params=pltpu.CompilerParams(
            collective_id=0, has_side_effects=True, vmem_limit_bytes=VMEM_ALL
        ),
        name="layer",
    )(mixed, tokens, gain[None, :], routes.T, shares.T, sgate, sup, sdown, gate, up, down)


def mixer_kernel(
    tokens_hbm,
    prior_hbm,
    gain_hbm,
    weight_hbm,
    decay_hbm,
    freq_hbm,
    step_hbm,
    imap_hbm,
    omap_hbm,
    skip_hbm,
    project_hbm,
    mixed_hbm,
    state_hbm,
    tokens_ref,
    old,
    gain_ref,
    weight,
    decay_ref,
    freq_ref,
    step_ref,
    imap_ref,
    omap_ref,
    skip_ref,
    project,
    active_ref,
    mixed,
    fresh,
    in_sem,
    out_sem,
    mixed_sem,
):
    S, D = tokens_ref.shape
    width = weight.shape[1]
    groups, entries = decay_ref.shape
    members = width // groups
    f4, bf = jnp.float32, jnp.bfloat16
    lane_groups = LANES // entries
    block = LANES // members
    cols = block * entries

    fetched = {}
    for i, (name, src, dst) in enumerate(
        (
            ("tokens", tokens_hbm, tokens_ref),
            ("gain", gain_hbm, gain_ref),
            ("step", step_hbm, step_ref),
            ("decay", decay_hbm, decay_ref),
            ("freq", freq_hbm, freq_ref),
            ("weight", weight_hbm, weight),
            ("imap", imap_hbm, imap_ref),
            ("old", prior_hbm, old),
            ("skip", skip_hbm, skip_ref),
            ("omap", omap_hbm, omap_ref),
            ("project", project_hbm, project),
        )
    ):
        fetched[name] = pltpu.make_async_copy(src, dst, in_sem.at[i])
        fetched[name].start()

    def state_copy(part, q):
        lanes = pl.ds(q * cols, cols)
        return pltpu.make_async_copy(fresh.at[part, :, lanes], state_hbm.at[part, :, lanes], out_sem.at[part, q])

    for name in ("step", "decay", "freq"):
        fetched[name].wait()

    eye = lax.broadcasted_iota(jnp.int32, (groups, groups), 0) == lax.broadcasted_iota(jnp.int32, (groups, groups), 1)
    log_column = jnp.sum(jnp.where(eye, step_ref[...], 0.0), axis=1, keepdims=True)
    step_size = jnp.exp(log_column)
    real_rate = -decay_ref[...]
    frequency = freq_ref[...]
    magnitude = jnp.exp(real_rate * step_size)
    turn_real = magnitude * jnp.cos(frequency * step_size)
    turn_imag = magnitude * jnp.sin(frequency * step_size)
    denominator = real_rate * real_rate + frequency * frequency
    hold_real = ((turn_real - 1.0) * real_rate + turn_imag * frequency) / denominator
    hold_imag = (turn_imag * real_rate - (turn_real - 1.0) * frequency) / denominator
    doubled = [jnp.concatenate([v] * lane_groups, axis=1) for v in (turn_real, turn_imag, hold_real, hold_imag)]
    row_group = lax.broadcasted_iota(jnp.int32, (groups, LANES), 0)
    lane_group = lax.broadcasted_iota(jnp.int32, (groups, LANES), 1) // entries

    fetched["tokens"].wait()
    fetched["gain"].wait()
    values = tokens_ref[...].astype(f4)
    factor = lax.rsqrt(jnp.mean(values * values, axis=-1, keepdims=True) + norm_eps)
    normed = (values * factor * gain_ref[...]).astype(bf)
    fetched["weight"].wait()
    drive = jnp.dot(normed, weight[...], preferred_element_type=f4).astype(bf)
    for name in ("imap", "old", "skip", "omap"):
        fetched[name].wait()

    in_row = lax.broadcasted_iota(jnp.int32, (LANES, LANES), 0) // members
    in_lane = lax.broadcasted_iota(jnp.int32, (LANES, LANES), 1) // entries
    out_row = lax.broadcasted_iota(jnp.int32, (LANES, 2 * LANES), 0) // members
    out_lane = lax.broadcasted_iota(jnp.int32, (LANES, 2 * LANES), 1) // entries

    for q in range(width // LANES):
        channels = slice(q * LANES, (q + 1) * LANES)
        mine = drive[:, channels]
        maps = [jnp.concatenate([imap_ref[part, channels, :]] * lane_groups, axis=1) for part in range(2)]
        outs = [jnp.concatenate([omap_ref[part, channels, :]] * (2 * lane_groups), axis=1) for part in range(2)]
        readout = mine.astype(f4) * skip_ref[:, channels]
        for m in range(cols // LANES):
            mask = in_row == in_lane + m * lane_groups
            both = jnp.concatenate([jnp.where(mask, v, 0.0) for v in maps], axis=1).astype(bf)
            push = jnp.dot(mine, both, preferred_element_type=f4)
            push_real, push_imag = push[:, :LANES], push[:, LANES:]
            first = q * block + m * lane_groups
            tr, ti, hr, hi = [
                jnp.sum(jnp.where(row_group == lane_group + first, v, 0.0), axis=0, keepdims=True) for v in doubled
            ]
            at = slice(q * cols + m * LANES, q * cols + (m + 1) * LANES)
            old_real, old_imag = old[0, :, at], old[1, :, at]
            fresh[0, :, at] = tr * old_real - ti * old_imag + (push_real * hr - push_imag * hi)
            fresh[1, :, at] = tr * old_imag + ti * old_real + (push_real * hi + push_imag * hr)
        state_copy(0, q).start()
        state_copy(1, q).start()
        for h in range(cols // (2 * LANES)):
            at = slice(q * cols + h * 2 * LANES, q * cols + (h + 1) * 2 * LANES)
            mask = out_row == out_lane + h * 2 * lane_groups
            for part in range(2):
                spread_out = jnp.where(mask, outs[part] if part == 0 else -outs[part], 0.0).astype(bf)
                readout = readout + lax.dot_general(
                    fresh[part, :, at].astype(bf), spread_out, (((1,), (1,)), ((), ())), preferred_element_type=f4
                )
        active_ref[:, channels] = jax.nn.gelu(readout).astype(bf)
    fetched["project"].wait()
    quarter = D // 4
    sent = []
    for h in range(4):
        at = slice(h * quarter, (h + 1) * quarter)
        mixed[:, at] = jnp.dot(active_ref[...], project[:, at], preferred_element_type=f4).astype(bf)
        sent.append(pltpu.make_async_copy(mixed.at[:, at], mixed_hbm.at[:, at], mixed_sem.at[h]))
        sent[-1].start()
    for copy in sent:
        copy.wait()
    for q in range(width // LANES):
        for part in range(2):
            state_copy(part, q).wait()


def mixer(tokens, prior, gain, weight, decay, freq, log_step, imap, omap, skip, project):
    S, D = tokens.shape
    width = weight.shape[1]
    f4 = jnp.float32
    hb = pl.BlockSpec(memory_space=pl.ANY)
    dma = pltpu.SemaphoreType.DMA
    by_channel = (2, width, imap.shape[2])
    return pl.pallas_call(
        mixer_kernel,
        out_shape=(
            jax.ShapeDtypeStruct((S, D), jnp.bfloat16),
            jax.ShapeDtypeStruct(prior.shape, jnp.float32),
        ),
        in_specs=[hb] * 11,
        out_specs=(hb, hb),
        scratch_shapes=[
            pltpu.VMEM((S, D), tokens.dtype),
            pltpu.VMEM(prior.shape, f4),
            pltpu.VMEM((1, D), f4),
            pltpu.VMEM(weight.shape, weight.dtype),
            pltpu.VMEM(decay.shape, f4),
            pltpu.VMEM(freq.shape, f4),
            pltpu.VMEM((1, log_step.shape[0]), f4),
            pltpu.VMEM(by_channel, f4),
            pltpu.VMEM(by_channel, f4),
            pltpu.VMEM((1, width), f4),
            pltpu.VMEM(project.shape, project.dtype),
            pltpu.VMEM((S, width), tokens.dtype),
            pltpu.VMEM((S, D), tokens.dtype),
            pltpu.VMEM(prior.shape, f4),
            dma((11,)),
            dma((2, width // LANES)),
            dma((4,)),
        ],
        compiler_params=pltpu.CompilerParams(vmem_limit_bytes=VMEM_ALL),
        name="mixer",
    )(
        tokens,
        prior,
        gain[None, :],
        weight,
        decay,
        freq,
        log_step[None, :],
        jnp.swapaxes(imap, 2, 3).reshape(by_channel),
        omap.reshape(by_channel),
        skip[None, :],
        project,
    )


def body(
    tokens,
    prior_state,
    mix_gain,
    in_weight,
    decay_rate,
    frequency,
    log_step,
    input_map,
    output_map,
    skip_gain,
    out_weight,
    channel_gain,
    expert_gate,
    expert_up,
    expert_down,
    shared_gate,
    shared_up,
    shared_down,
    routes,
    route_weights,
):
    mixed, new_state = mixer(
        tokens,
        prior_state,
        mix_gain,
        in_weight,
        decay_rate,
        frequency,
        log_step,
        input_map,
        output_map,
        skip_gain,
        out_weight,
    )
    layer_out = layer(
        mixed,
        tokens,
        channel_gain,
        routes,
        route_weights,
        shared_gate,
        shared_up,
        shared_down,
        expert_gate,
        expert_up,
        expert_down,
    )
    return (layer_out, new_state)


def solution(mesh):
    in_specs = (
        P(("grp", "ep"), None),
        P(None, ("grp", "ep"), "tp"),
        P(),
        P(None, "tp"),
        P("tp", None),
        P("tp", None),
        P("tp"),
        P(None, "tp", None, None),
        P(None, "tp", None, None),
        P("tp"),
        P("tp", None),
        P(),
        P("ep", None, "tp"),
        P("ep", None, "tp"),
        P("ep", "tp", None),
        P(None, "tp"),
        P(None, "tp"),
        P("tp", None),
        P(("grp", "ep"), None),
        P(("grp", "ep"), None),
    )
    out_specs = (P(("grp", "ep"), "tp"), P(None, ("grp", "ep"), "tp"))
    return jax.shard_map(body, mesh=mesh, in_specs=in_specs, out_specs=out_specs, check_vma=False)
```

```python
import functools

import jax
import jax.numpy as jnp
from jax import lax
from jax.experimental import pallas as pl
from jax.experimental.pallas import tpu as pltpu
from jax.sharding import PartitionSpec as P

MESH = pl.DeviceIdType.MESH
norm_eps = 1e-06
ROW_RING = 4
CHUNKS = 4
LANES = 128
VMEM_ALL = 63 * 1024 * 1024


def layer_kernel(
    cfg,
    mixed_hbm,
    tokens_hbm,
    gain_hbm,
    routes_hbm,
    shares_hbm,
    sgate_hbm,
    sup_hbm,
    sdown_hbm,
    gate_hbm,
    up_hbm,
    down_hbm,
    out_ref,
    tokens_ref,
    gain_ref,
    routes_ref,
    shares_ref,
    table,
    mixed,
    mixed_in,
    middle,
    normed,
    s_in,
    s_out,
    s_hidden,
    s_part,
    s_part_in,
    gathered,
    tables,
    pick,
    spread,
    staged,
    rows_in,
    w_in,
    w_out,
    partial,
    partner_part,
    total,
    back,
    sums_in,
    sums_out,
    far_pick,
    far_spread,
    far_staged,
    far_back,
    w_sem,
    m_sem,
    s_sem,
    t_send,
    t_recv,
    z_send,
    z_recv,
    x_send,
    x_recv,
    c_send,
    c_recv,
    p_send,
    p_recv,
    b_send,
    b_recv,
    r_send,
    r_recv,
    f_send,
    f_recv,
    g_send,
):
    Z, X, S, H, R, nc, top = cfg
    W = H // nc
    half = Z // 2
    F = gate_hbm.shape[2]
    SF = sgate_hbm.shape[1]
    ep = lax.axis_index("ep")
    tp = lax.axis_index("tp")
    other = 1 - tp
    z, x = ep // X, lax.rem(ep, X)

    def at_z(offset):
        return {"ep": lax.rem(z + offset + Z, Z) * X + x}

    def at_x(offset):
        return {"ep": z * X + lax.rem(x + offset + X, X)}

    def at_far(dz, dx):
        return {"ep": lax.rem(z + dz + Z, Z) * X + lax.rem(x + dx + X, X)}

    partner = {"tp": other}
    hc = nc // 2

    def send(src, dst, s_sem, r_sem, device):
        return pltpu.make_async_remote_copy(
            src_ref=src, dst_ref=dst, send_sem=s_sem, recv_sem=r_sem,
            device_id=device, device_id_type=MESH,
        )

    def shared_copies():
        return (
            pltpu.make_async_copy(sgate_hbm, s_in.at[:, pl.ds(0, SF)], w_sem.at[1]),
            pltpu.make_async_copy(sup_hbm, s_in.at[:, pl.ds(SF, SF)], w_sem.at[2]),
            pltpu.make_async_copy(sdown_hbm, s_out, w_sem.at[3]),
        )

    def expert_copies():
        return (
            pltpu.make_async_copy(gate_hbm.at[0], w_in.at[:, pl.ds(0, F)], w_sem.at[4]),
            pltpu.make_async_copy(up_hbm.at[0], w_in.at[:, pl.ds(F, F)], w_sem.at[5]),
            pltpu.make_async_copy(down_hbm.at[0], w_out, w_sem.at[6]),
        )

    small = [
        pltpu.make_async_copy(src, dst, w_sem.at[7 + i])
        for i, (src, dst) in enumerate(
            (
                (mixed_hbm, mixed),
                (routes_hbm, routes_ref),
                (shares_hbm, shares_ref),
                (tokens_hbm, tokens_ref),
                (gain_hbm, gain_ref),
            )
        )
    ]
    for copy in small:
        copy.start()

    barrier = pltpu.get_barrier_semaphore()
    for device in (*[at_far(s, d) for s in (1, -1) for d in range(X)], *[at_x(d) for d in range(1, X)], partner):
        pl.semaphore_signal(barrier, inc=1, device_id=device, device_id_type=MESH)

    table[...] = jnp.where(lax.broadcasted_iota(jnp.int32, (16, LANES), 0) < 8, -1.0, 0.0)
    for copy in small[:3]:
        copy.wait()
    table[pl.ds(0, top), pl.ds(0, S)] = routes_ref[...].astype(jnp.float32)
    table[pl.ds(8, top), pl.ds(0, S)] = shares_ref[...]
    tables[0] = table[...].astype(jnp.bfloat16)
    for copy in (*shared_copies(), *expert_copies()):
        copy.start()
    pl.semaphore_wait(barrier, 3 * X)

    mixed_copy = send(mixed, mixed_in, m_sem.at[0], m_sem.at[1], partner)
    mixed_copy.start()

    def t_copy(way, k):
        if way == 0:
            return send(tables.at[k], tables.at[k + 1], t_send.at[0, k], t_recv.at[k + 1], at_z(1))
        r = lax.rem(Z - k, Z)
        return send(tables.at[r], tables.at[Z - k - 1], t_send.at[1, k], t_recv.at[Z - k - 1], at_z(-1))

    def t_stage(k):
        for way in (0, 1):
            limit = half - 1

            @pl.when((k >= 1) & (k <= limit))
            def _():
                t_copy(way, k - 1).wait_recv()

            @pl.when(k + 1 <= limit)
            def _():
                t_copy(way, k).start()

    def z_copy(way, k, c):
        if way == 0:
            return send(gathered.at[k, c], gathered.at[k + 1, c], z_send.at[0, k, c], z_recv.at[k + 1, c], at_z(1))
        r = lax.rem(Z - k, Z)
        return send(gathered.at[r, c], gathered.at[Z - k - 1, c], z_send.at[1, k, c], z_recv.at[Z - k - 1, c], at_z(-1))

    def z_stage(k, c):
        for way in (0, 1):
            limit = half - 1

            @pl.when((k >= 1) & (k <= limit))
            def _():
                z_copy(way, k - 1, c).wait_recv()

            @pl.when(k + 1 <= limit)
            def _():
                z_copy(way, k, c).start()

    before = (
        lax.broadcasted_iota(jnp.int32, (LANES, LANES), 0) < lax.broadcasted_iota(jnp.int32, (LANES, LANES), 1)
    ).astype(jnp.float32).astype(jnp.bfloat16)
    offset = lax.broadcasted_iota(jnp.int32, (8, LANES), 0)
    column = offset + x
    column = jnp.where(column >= X, column - X, column)

    def experts_at(dz):
        return jnp.where(offset < X, lax.rem(z + dz + Z, Z) * X + column, -2).astype(jnp.float32)

    def build(r):
        build_for(r, experts_at(0), pick.at[r], spread.at[r])

    def build_for(r, expert_of, pick_ref, spread_ref):
        table = tables[r].astype(jnp.float32)
        named = jnp.zeros((8, LANES), jnp.float32)
        weight = jnp.zeros((8, LANES), jnp.float32)
        for k in range(top):
            hit = table[k : k + 1, :] == expert_of
            named = named + jnp.where(hit, 1.0, 0.0)
            weight = weight + jnp.where(hit, table[8 + k : 9 + k, :], 0.0)
        rank = jnp.dot(named.astype(jnp.bfloat16), before, preferred_element_type=jnp.float32)
        code = jnp.where(named > 0.0, rank, -1.0)
        slot = lax.broadcasted_iota(jnp.int32, (R, LANES), 0).astype(jnp.float32)
        parts, weighted = [], []
        for d in range(X):
            block = jnp.where(code[d : d + 1, :] == slot, 1.0, 0.0)
            parts.append(block)
            weighted.append(block * weight[d : d + 1, :])
        pick_ref[...] = jnp.concatenate(parts, axis=0).astype(jnp.bfloat16)
        spread_ref[...] = jnp.concatenate(weighted, axis=0).T.astype(jnp.bfloat16)

    t_stage(jnp.int32(0))
    build(0)

    for copy in small[3:]:
        copy.wait()
    mixed_copy.wait_recv()
    both = mixed[...].astype(jnp.float32) + mixed_in[...].astype(jnp.float32)
    middle[...] = (tokens_ref[...].astype(jnp.float32) + both).astype(jnp.bfloat16)
    values = middle[...].astype(jnp.float32)
    factor = lax.rsqrt(jnp.mean(values * values, axis=-1, keepdims=True) + norm_eps)
    normed[...] = (values * factor * gain_ref[...]).astype(jnp.bfloat16)

    def own(c):
        return pl.ds(pl.multiple_of(tp * H + c * W, W), W)

    for c in range(nc):
        gathered[0, c] = normed[:, own(c)]
        z_stage(jnp.int32(0), c)

    def shared_hidden():
        for copy in shared_copies():
            copy.wait()
        acc = jnp.dot(normed[...], s_in[...], preferred_element_type=jnp.float32)
        s_hidden[...] = (jax.nn.silu(acc[:, :SF]) * acc[:, SF:]).astype(jnp.bfloat16)

    s_copy = send(s_part.at[other], s_part_in, s_sem.at[0], s_sem.at[1], partner)

    def shared_partial():
        for h in range(2):
            for c in range(nc):
                s_part[h, :, pl.ds(c * W, W)] = jnp.dot(
                    s_hidden[...], s_out[:, pl.ds(h * H + c * W, W)], preferred_element_type=jnp.float32
                ).astype(jnp.bfloat16)
        s_copy.start()

    def x_copy(r, d, c):
        rows = pl.ds(d * R, R)
        return send(staged.at[r, c, rows, :], rows_in.at[r, tp, c, rows, :], x_send.at[r], x_recv.at[r], at_x(d))

    def c_copy(r):
        return send(rows_in.at[r, tp], rows_in.at[r, tp], c_send.at[r], c_recv.at[r], partner)

    def p_copy(r):
        return send(partial.at[r, other], partner_part.at[r], p_send.at[r], p_recv.at[r], partner)

    def b_copy(r, d, c):
        rows = pl.ds(d * R, R)
        return send(total.at[r, c, rows, :], back.at[r, c, rows, :], b_send.at[r], b_recv.at[r, c], at_x(-d))

    def select(r, c):
        chosen = jnp.dot(
            pick[r, :, pl.ds(0, S)], gathered[r, c], preferred_element_type=jnp.float32
        ).astype(jnp.bfloat16)
        rows_in[r, tp, c, pl.ds(0, R), :] = chosen[:R]
        staged[r, c] = chosen
        for d in range(1, X):
            x_copy(r, d, c).start()

    def far_row(way):
        return half - 1 if way == 0 else Z - half + 1

    def far_chunks(way):
        return pl.ds(way * hc, hc)

    def f_copy(way, d, c):
        rows = pl.ds(d * R, R)
        return send(
            far_staged.at[way, c, rows, :],
            rows_in.at[half, tp, way * hc + c, rows, :],
            f_send.at[way],
            x_recv.at[half],
            at_far(1 - 2 * way, d),
        )

    def g_copy(way, d, c):
        rows = pl.ds(d * R, R)
        return send(
            total.at[half, way * hc + c, rows, :],
            far_back.at[way, c, rows, :],
            g_send.at[way],
            f_recv.at[way, c],
            at_far(2 * way - 1, -d),
        )

    def select_far(c):
        way = c // hc
        far_staged[way, c - way * hc] = jnp.dot(
            far_pick[way, :, pl.ds(0, S)], gathered[far_row(way), c], preferred_element_type=jnp.float32
        ).astype(jnp.bfloat16)
        for d in range(X):
            f_copy(way, d, c - way * hc).start()

    def hand_far():
        send(rows_in.at[half, tp], rows_in.at[half, tp], f_send.at[0], x_recv.at[half], partner).wait_recv()
        c_copy(half).start()

    rest = pl.ds(R, (X - 1) * R)

    def hand_over(r):
        send(staged.at[r, :, rest, :], rows_in.at[r, tp, :, rest, :], x_send.at[r], x_recv.at[r], at_x(1)).wait_recv()
        c_copy(r).start()

    def expert(rs):
        M = X * R
        for r in rs:
            send(rows_in.at[r, other], rows_in.at[r, other], c_send.at[r], c_recv.at[r], partner).wait_recv()
        acc = jnp.zeros((len(rs) * M, 2 * F), jnp.float32)
        for h in range(2):
            for c in range(nc):
                rows = jnp.concatenate([rows_in[r, h, c] for r in rs], axis=0)
                acc = acc + jnp.dot(rows, w_in[pl.ds(h * H + c * W, W), :], preferred_element_type=jnp.float32)
        hidden = (jax.nn.silu(acc[:, :F]) * acc[:, F:]).astype(jnp.bfloat16)
        for h in range(2):
            for c in range(nc):
                piece = jnp.dot(
                    hidden, w_out[:, pl.ds(h * H + c * W, W)], preferred_element_type=jnp.float32
                ).astype(jnp.bfloat16)
                for n, r in enumerate(rs):
                    partial[r, h, c] = piece[n * M : (n + 1) * M]
        for r in rs:
            p_copy(r).start()

    def join(r):
        p_copy(r).wait_recv()
        for c in range(nc):
            join_chunk(r, c)

    def join_chunk(r, c):
        y = (partial[r, tp, c].astype(jnp.float32) + partner_part[r, c].astype(jnp.float32)).astype(jnp.bfloat16)
        back[r, c, pl.ds(0, R), :] = y[:R]
        total[r, c] = y

    def hand_back(r):
        for c in range(nc):
            for d in range(1, X):
                b_copy(r, d, c).start()

    def of_pair(stage, k, way, least=0):
        if way == 0:
            @pl.when((k >= least) & (k < half))
            def _():
                stage(k)
        else:
            @pl.when((k >= 1) & (k < half))
            def _():
                stage(Z - k)

    def step(i, carry):
        @pl.when(i < half)
        def _():
            t_stage(i)

        of_pair(build, i, 0, 1)
        of_pair(build, i, 1, 1)

        @pl.when(i == half - 1)
        def _():
            for way in (0, 1):
                build_for(far_row(way), experts_at(1 - 2 * way), far_pick.at[way], far_spread.at[way])

        for c in range(nc):
            z_stage(i, c)

            @pl.when(i == half - 1)
            def _():
                select_far(c)

            of_pair(functools.partial(select, c=c), i, 0, 1)
            of_pair(functools.partial(select, c=c), i, 1, 1)
            if c == 1:

                @pl.when(i == 2)
                def _():
                    for copy in expert_copies():
                        copy.wait()
                    expert([0])

                @pl.when(i > 2)
                def _():
                    expert([i - 2, Z - i + 2])

            if c == 2:
                of_pair(join, i - 3, 0)
                of_pair(join, i - 3, 1)

        @pl.when(i == half)
        def _():
            hand_far()

        of_pair(hand_over, i - 1, 0)
        of_pair(hand_over, i - 1, 1)
        return carry

    for c in range(nc):
        select(0, c)
    lax.fori_loop(1, half + 1, step, 0)

    last = (half - 1, half + 1, half)
    expert(last)
    join(half - 2)
    if half > 2:
        join(half + 2)
    for r in last:
        p_copy(r).wait_recv()
    for c in range(nc):
        for r in last:
            join_chunk(r, c)
        for d in range(X):
            g_copy(c // hc, d, c - c // hc * hc).start()
        for d in range(1, X):
            b_copy(half - 1, d, c).start()
            b_copy(half + 1, d, c).start()
    hand_back(half - 2)
    if half > 2:
        hand_back(half + 2)
    shared_hidden()
    shared_partial()

    def r_copy(way, k, c):
        if way == 0:
            return send(sums_out.at[k, c], sums_in.at[k - 1, c], r_send.at[k, c], r_recv.at[k - 1, c], at_z(-1))
        return send(sums_out.at[Z - k, c], sums_in.at[Z - k + 1, c], r_send.at[Z - k, c], r_recv.at[Z - k + 1, c], at_z(1))

    def share_of(r, c):
        return jnp.dot(spread[r, pl.ds(0, S), :], back[r, c], preferred_element_type=jnp.float32)

    def back_wait(r, c):
        send(total.at[r, c, rest, :], back.at[r, c, rest, :], b_send.at[r], b_recv.at[r, c], at_x(1)).wait_recv()

    def go_back(i, carry):
        k = half - 1 - i
        of_pair(hand_back, k - 2, 0)
        of_pair(hand_back, k - 2, 1)
        for c in range(nc):
            back_wait(k, c)
            back_wait(Z - k, c)

            @pl.when(k == half - 1)
            def _():
                way, at = c // hc, c - c // hc * hc
                send(
                    far_staged.at[way, at], far_back.at[way, at], g_send.at[way], f_recv.at[way, at], partner
                ).wait_recv()

            for way in (0, 1):
                r = k if way == 0 else Z - k
                mine = share_of(r, c)

                @pl.when(k == half - 1)
                def _():
                    first = mine
                    if c // hc == way:
                        first = mine + jnp.dot(
                            far_spread[way, pl.ds(0, S), :],
                            far_back[way, c - way * hc],
                            preferred_element_type=jnp.float32,
                        )
                    sums_out[r, c] = first.astype(jnp.bfloat16)

                @pl.when(k < half - 1)
                def _():
                    r_copy(way, k + 1, c).wait_recv()
                    sums_out[r, c] = (mine + sums_in[r, c].astype(jnp.float32)).astype(jnp.bfloat16)

                r_copy(way, k, c).start()
        return carry

    lax.fori_loop(0, half - 1, go_back, 0)

    for c in range(nc):
        back_wait(0, c)
    s_copy.wait_recv()
    for c in range(nc):
        mine = share_of(0, c) + middle[:, own(c)].astype(jnp.float32)
        mine = mine + s_part[tp, :, pl.ds(c * W, W)].astype(jnp.float32)
        mine = mine + s_part_in[:, pl.ds(c * W, W)].astype(jnp.float32)
        r_copy(0, 1, c).wait_recv()
        r_copy(1, 1, c).wait_recv()
        mine = mine + sums_in[0, c].astype(jnp.float32) + sums_in[Z, c].astype(jnp.float32)
        out_ref[:, pl.ds(c * W, W)] = mine.astype(out_ref.dtype)

    mixed_copy.wait_send()
    s_copy.wait_send()

    def drain(k, carry):
        for way in (0, 1):
            t_copy(way, k).wait_send()
            for c in range(nc):
                z_copy(way, k, c).wait_send()
                r_copy(way, k + 1, c).wait_send()
        return carry

    lax.fori_loop(0, half - 1, drain, 0)

    def drain_rows(r, carry):
        @pl.when(r != half)
        def _():
            send(staged.at[r, :, rest, :], rows_in.at[r, tp, :, rest, :], x_send.at[r], x_recv.at[r], at_x(1)).wait_send()
            send(total.at[r, :, rest, :], back.at[r, :, rest, :], b_send.at[r], b_recv.at[r, 0], at_x(1)).wait_send()

        c_copy(r).wait_send()
        p_copy(r).wait_send()
        return carry

    lax.fori_loop(0, Z, drain_rows, 0)
    for way in (0, 1):
        send(far_staged.at[way], far_back.at[way], f_send.at[way], f_recv.at[way, 0], partner).wait_send()
        send(total.at[half, far_chunks(way)], far_back.at[way], g_send.at[way], f_recv.at[way, 0], partner).wait_send()


def layer(mixed, tokens, gain, routes, shares, sgate, sup, sdown, gate, up, down):
    top = routes.shape[1]
    S, D = tokens.shape
    H = D // lax.axis_size("tp")
    X = ROW_RING
    Z = lax.axis_size("ep") // X
    nc = CHUNKS
    W = H // nc
    R = 16
    F = gate.shape[2]
    SF = sgate.shape[1]
    bf = jnp.bfloat16
    dma = pltpu.SemaphoreType.DMA
    vm = pl.BlockSpec(memory_space=pltpu.VMEM)
    hb = pl.BlockSpec(memory_space=pl.ANY)
    return pl.pallas_call(
        functools.partial(layer_kernel, (Z, X, S, H, R, nc, top)),
        out_shape=jax.ShapeDtypeStruct((S, H), bf),
        in_specs=[hb] * 11,
        out_specs=vm,
        scratch_shapes=[
            pltpu.VMEM((S, D), bf),
            pltpu.VMEM((1, D), jnp.float32),
            pltpu.VMEM((top, S), jnp.int32),
            pltpu.VMEM((top, S), jnp.float32),
            pltpu.VMEM((16, LANES), jnp.float32),
            pltpu.VMEM((S, D), bf),
            pltpu.VMEM((S, D), bf),
            pltpu.VMEM((S, D), bf),
            pltpu.VMEM((S, D), bf),
            pltpu.VMEM((D, 2 * SF), bf),
            pltpu.VMEM((SF, D), bf),
            pltpu.VMEM((S, SF), bf),
            pltpu.VMEM((2, S, H), bf),
            pltpu.VMEM((S, H), bf),
            pltpu.VMEM((Z, nc, S, W), bf),
            pltpu.VMEM((Z, 16, LANES), bf),
            pltpu.VMEM((Z, X * R, LANES), bf),
            pltpu.VMEM((Z, LANES, X * R), bf),
            pltpu.VMEM((Z, nc, X * R, W), bf),
            pltpu.VMEM((Z, 2, nc, X * R, W), bf),
            pltpu.VMEM((D, 2 * F), bf),
            pltpu.VMEM((F, D), bf),
            pltpu.VMEM((Z, 2, nc, X * R, W), bf),
            pltpu.VMEM((Z, nc, X * R, W), bf),
            pltpu.VMEM((Z, nc, X * R, W), bf),
            pltpu.VMEM((Z, nc, X * R, W), bf),
            pltpu.VMEM((Z + 1, nc, S, W), bf),
            pltpu.VMEM((Z, nc, S, W), bf),
            pltpu.VMEM((2, X * R, LANES), bf),
            pltpu.VMEM((2, LANES, X * R), bf),
            pltpu.VMEM((2, nc // 2, X * R, W), bf),
            pltpu.VMEM((2, nc // 2, X * R, W), bf),
            dma((12,)),
            dma((2,)),
            dma((2,)),
            dma((2, Z // 2)),
            dma((Z,)),
            dma((2, Z // 2, nc)),
            dma((Z, nc)),
            dma((Z,)),
            dma((Z,)),
            dma((Z,)),
            dma((Z,)),
            dma((Z,)),
            dma((Z,)),
            dma((Z,)),
            dma((Z, nc)),
            dma((Z, nc)),
            dma((Z + 1, nc)),
            dma((2,)),
            dma((2, nc // 2)),
            dma((2,)),
        ],
        compiler_params=pltpu.CompilerParams(
            collective_id=0, has_side_effects=True, vmem_limit_bytes=VMEM_ALL
        ),
        name="layer",
    )(mixed, tokens, gain[None, :], routes.T, shares.T, sgate, sup, sdown, gate, up, down)


def mixer_kernel(
    tokens_hbm,
    prior_hbm,
    gain_hbm,
    weight_hbm,
    decay_hbm,
    freq_hbm,
    step_hbm,
    imap_hbm,
    omap_hbm,
    skip_hbm,
    project_hbm,
    mixed_hbm,
    state_hbm,
    tokens_ref,
    old,
    gain_ref,
    weight,
    decay_ref,
    freq_ref,
    step_ref,
    imap_ref,
    omap_ref,
    skip_ref,
    project,
    active_ref,
    mixed,
    fresh,
    in_sem,
    out_sem,
    mixed_sem,
):
    S, D = tokens_ref.shape
    width = weight.shape[1]
    groups, entries = decay_ref.shape
    members = width // groups
    f4, bf = jnp.float32, jnp.bfloat16
    lane_groups = LANES // entries
    block = LANES // members
    cols = block * entries

    fetched = {}
    for i, (name, src, dst) in enumerate(
        (
            ("tokens", tokens_hbm, tokens_ref),
            ("gain", gain_hbm, gain_ref),
            ("step", step_hbm, step_ref),
            ("decay", decay_hbm, decay_ref),
            ("freq", freq_hbm, freq_ref),
            ("weight", weight_hbm, weight),
            ("imap", imap_hbm, imap_ref),
            ("old", prior_hbm, old),
            ("skip", skip_hbm, skip_ref),
            ("omap", omap_hbm, omap_ref),
            ("project", project_hbm, project),
        )
    ):
        fetched[name] = pltpu.make_async_copy(src, dst, in_sem.at[i])
        fetched[name].start()

    def state_copy(part, q):
        lanes = pl.ds(q * cols, cols)
        return pltpu.make_async_copy(fresh.at[part, :, lanes], state_hbm.at[part, :, lanes], out_sem.at[part, q])

    for name in ("step", "decay", "freq"):
        fetched[name].wait()

    eye = lax.broadcasted_iota(jnp.int32, (groups, groups), 0) == lax.broadcasted_iota(jnp.int32, (groups, groups), 1)
    log_column = jnp.sum(jnp.where(eye, step_ref[...], 0.0), axis=1, keepdims=True)
    step_size = jnp.exp(log_column)
    real_rate = -decay_ref[...]
    frequency = freq_ref[...]
    magnitude = jnp.exp(real_rate * step_size)
    turn_real = magnitude * jnp.cos(frequency * step_size)
    turn_imag = magnitude * jnp.sin(frequency * step_size)
    denominator = real_rate * real_rate + frequency * frequency
    hold_real = ((turn_real - 1.0) * real_rate + turn_imag * frequency) / denominator
    hold_imag = (turn_imag * real_rate - (turn_real - 1.0) * frequency) / denominator
    doubled = [jnp.concatenate([v] * lane_groups, axis=1) for v in (turn_real, turn_imag, hold_real, hold_imag)]
    row_group = lax.broadcasted_iota(jnp.int32, (groups, LANES), 0)
    lane_group = lax.broadcasted_iota(jnp.int32, (groups, LANES), 1) // entries

    fetched["tokens"].wait()
    fetched["gain"].wait()
    values = tokens_ref[...].astype(f4)
    factor = lax.rsqrt(jnp.mean(values * values, axis=-1, keepdims=True) + norm_eps)
    normed = (values * factor * gain_ref[...]).astype(bf)
    fetched["weight"].wait()
    drive = jnp.dot(normed, weight[...], preferred_element_type=f4).astype(bf)
    for name in ("imap", "old", "skip", "omap"):
        fetched[name].wait()

    in_row = lax.broadcasted_iota(jnp.int32, (LANES, LANES), 0) // members
    in_lane = lax.broadcasted_iota(jnp.int32, (LANES, LANES), 1) // entries
    out_row = lax.broadcasted_iota(jnp.int32, (LANES, 2 * LANES), 0) // members
    out_lane = lax.broadcasted_iota(jnp.int32, (LANES, 2 * LANES), 1) // entries

    for q in range(width // LANES):
        channels = slice(q * LANES, (q + 1) * LANES)
        mine = drive[:, channels]
        maps = [jnp.concatenate([imap_ref[part, channels, :]] * lane_groups, axis=1) for part in range(2)]
        outs = [jnp.concatenate([omap_ref[part, channels, :]] * (2 * lane_groups), axis=1) for part in range(2)]
        readout = mine.astype(f4) * skip_ref[:, channels]
        for m in range(cols // LANES):
            mask = in_row == in_lane + m * lane_groups
            both = jnp.concatenate([jnp.where(mask, v, 0.0) for v in maps], axis=1).astype(bf)
            push = jnp.dot(mine, both, preferred_element_type=f4)
            push_real, push_imag = push[:, :LANES], push[:, LANES:]
            first = q * block + m * lane_groups
            tr, ti, hr, hi = [
                jnp.sum(jnp.where(row_group == lane_group + first, v, 0.0), axis=0, keepdims=True) for v in doubled
            ]
            at = slice(q * cols + m * LANES, q * cols + (m + 1) * LANES)
            old_real, old_imag = old[0, :, at], old[1, :, at]
            fresh[0, :, at] = tr * old_real - ti * old_imag + (push_real * hr - push_imag * hi)
            fresh[1, :, at] = tr * old_imag + ti * old_real + (push_real * hi + push_imag * hr)
        state_copy(0, q).start()
        state_copy(1, q).start()
        for h in range(cols // (2 * LANES)):
            at = slice(q * cols + h * 2 * LANES, q * cols + (h + 1) * 2 * LANES)
            mask = out_row == out_lane + h * 2 * lane_groups
            for part in range(2):
                spread_out = jnp.where(mask, outs[part] if part == 0 else -outs[part], 0.0).astype(bf)
                readout = readout + lax.dot_general(
                    fresh[part, :, at].astype(bf), spread_out, (((1,), (1,)), ((), ())), preferred_element_type=f4
                )
        active_ref[:, channels] = jax.nn.gelu(readout).astype(bf)
    fetched["project"].wait()
    quarter = D // 4
    sent = []
    for h in range(4):
        at = slice(h * quarter, (h + 1) * quarter)
        mixed[:, at] = jnp.dot(active_ref[...], project[:, at], preferred_element_type=f4).astype(bf)
        sent.append(pltpu.make_async_copy(mixed.at[:, at], mixed_hbm.at[:, at], mixed_sem.at[h]))
        sent[-1].start()
    for copy in sent:
        copy.wait()
    for q in range(width // LANES):
        for part in range(2):
            state_copy(part, q).wait()


def mixer(tokens, prior, gain, weight, decay, freq, log_step, imap, omap, skip, project):
    S, D = tokens.shape
    width = weight.shape[1]
    f4 = jnp.float32
    hb = pl.BlockSpec(memory_space=pl.ANY)
    dma = pltpu.SemaphoreType.DMA
    by_channel = (2, width, imap.shape[2])
    return pl.pallas_call(
        mixer_kernel,
        out_shape=(
            jax.ShapeDtypeStruct((S, D), jnp.bfloat16),
            jax.ShapeDtypeStruct(prior.shape, jnp.float32),
        ),
        in_specs=[hb] * 11,
        out_specs=(hb, hb),
        scratch_shapes=[
            pltpu.VMEM((S, D), tokens.dtype),
            pltpu.VMEM(prior.shape, f4),
            pltpu.VMEM((1, D), f4),
            pltpu.VMEM(weight.shape, weight.dtype),
            pltpu.VMEM(decay.shape, f4),
            pltpu.VMEM(freq.shape, f4),
            pltpu.VMEM((1, log_step.shape[0]), f4),
            pltpu.VMEM(by_channel, f4),
            pltpu.VMEM(by_channel, f4),
            pltpu.VMEM((1, width), f4),
            pltpu.VMEM(project.shape, project.dtype),
            pltpu.VMEM((S, width), tokens.dtype),
            pltpu.VMEM((S, D), tokens.dtype),
            pltpu.VMEM(prior.shape, f4),
            dma((11,)),
            dma((2, width // LANES)),
            dma((4,)),
        ],
        compiler_params=pltpu.CompilerParams(vmem_limit_bytes=VMEM_ALL),
        name="mixer",
    )(
        tokens,
        prior,
        gain[None, :],
        weight,
        decay,
        freq,
        log_step[None, :],
        jnp.swapaxes(imap, 2, 3).reshape(by_channel),
        omap.reshape(by_channel),
        skip[None, :],
        project,
    )


def body(
    tokens,
    prior_state,
    mix_gain,
    in_weight,
    decay_rate,
    frequency,
    log_step,
    input_map,
    output_map,
    skip_gain,
    out_weight,
    channel_gain,
    expert_gate,
    expert_up,
    expert_down,
    shared_gate,
    shared_up,
    shared_down,
    routes,
    route_weights,
):
    mixed, new_state = mixer(
        tokens,
        prior_state,
        mix_gain,
        in_weight,
        decay_rate,
        frequency,
        log_step,
        input_map,
        output_map,
        skip_gain,
        out_weight,
    )
    layer_out = layer(
        mixed,
        tokens,
        channel_gain,
        routes,
        route_weights,
        shared_gate,
        shared_up,
        shared_down,
        expert_gate,
        expert_up,
        expert_down,
    )
    return (layer_out, new_state)


def solution(mesh):
    in_specs = (
        P(("grp", "ep"), None),
        P(None, ("grp", "ep"), "tp"),
        P(),
        P(None, "tp"),
        P("tp", None),
        P("tp", None),
        P("tp"),
        P(None, "tp", None, None),
        P(None, "tp", None, None),
        P("tp"),
        P("tp", None),
        P(),
        P("ep", None, "tp"),
        P("ep", None, "tp"),
        P("ep", "tp", None),
        P(None, "tp"),
        P(None, "tp"),
        P("tp", None),
        P(("grp", "ep"), None),
        P(("grp", "ep"), None),
    )
    out_specs = (P(("grp", "ep"), "tp"), P(None, ("grp", "ep"), "tp"))
    return jax.shard_map(body, mesh=mesh, in_specs=in_specs, out_specs=out_specs, check_vma=False)
```

```python
import functools

import jax
import jax.numpy as jnp
from jax import lax
from jax.experimental import pallas as pl
from jax.experimental.pallas import tpu as pltpu
from jax.sharding import PartitionSpec as P

MESH = pl.DeviceIdType.MESH
norm_eps = 1e-06
ROW_RING = 4
CHUNKS = 4
LANES = 128
VMEM_ALL = 63 * 1024 * 1024


def layer_kernel(
    cfg,
    mixed_hbm,
    tokens_hbm,
    gain_hbm,
    routes_hbm,
    shares_hbm,
    sgate_hbm,
    sup_hbm,
    sdown_hbm,
    gate_hbm,
    up_hbm,
    down_hbm,
    out_ref,
    tokens_ref,
    gain_ref,
    routes_ref,
    shares_ref,
    table,
    mixed,
    mixed_in,
    middle,
    normed,
    s_in,
    s_out,
    s_hidden,
    s_part,
    s_part_in,
    gathered,
    tables,
    pick,
    spread,
    staged,
    rows_in,
    w_in,
    w_out,
    partial,
    partner_part,
    total,
    back,
    sums_in,
    sums_out,
    far_pick,
    far_spread,
    far_staged,
    far_back,
    w_sem,
    m_sem,
    s_sem,
    t_send,
    t_recv,
    z_send,
    z_recv,
    x_send,
    x_recv,
    c_send,
    c_recv,
    p_send,
    p_recv,
    b_send,
    b_recv,
    r_send,
    r_recv,
    f_send,
    f_recv,
    g_send,
    near_sem,
    far_sem,
):
    Z, X, S, H, R, nc, top = cfg
    W = H // nc
    half = Z // 2
    F = gate_hbm.shape[2]
    SF = sgate_hbm.shape[1]
    ep = lax.axis_index("ep")
    tp = lax.axis_index("tp")
    other = 1 - tp
    z, x = ep // X, lax.rem(ep, X)

    def at_z(offset):
        return {"ep": lax.rem(z + offset + Z, Z) * X + x}

    def at_x(offset):
        return {"ep": z * X + lax.rem(x + offset + X, X)}

    def at_far(dz, dx):
        return {"ep": lax.rem(z + dz + Z, Z) * X + lax.rem(x + dx + X, X)}

    partner = {"tp": other}
    hc = nc // 2

    def send(src, dst, s_sem, r_sem, device):
        return pltpu.make_async_remote_copy(
            src_ref=src, dst_ref=dst, send_sem=s_sem, recv_sem=r_sem,
            device_id=device, device_id_type=MESH,
        )

    def shared_copies():
        return (
            pltpu.make_async_copy(sgate_hbm, s_in.at[:, pl.ds(0, SF)], w_sem.at[1]),
            pltpu.make_async_copy(sup_hbm, s_in.at[:, pl.ds(SF, SF)], w_sem.at[2]),
            pltpu.make_async_copy(sdown_hbm, s_out, w_sem.at[3]),
        )

    def expert_copies():
        return (
            pltpu.make_async_copy(gate_hbm.at[0], w_in.at[:, pl.ds(0, F)], w_sem.at[4]),
            pltpu.make_async_copy(up_hbm.at[0], w_in.at[:, pl.ds(F, F)], w_sem.at[5]),
            pltpu.make_async_copy(down_hbm.at[0], w_out, w_sem.at[6]),
        )

    small = [
        pltpu.make_async_copy(src, dst, w_sem.at[7 + i])
        for i, (src, dst) in enumerate(
            (
                (mixed_hbm, mixed),
                (routes_hbm, routes_ref),
                (shares_hbm, shares_ref),
                (tokens_hbm, tokens_ref),
                (gain_hbm, gain_ref),
            )
        )
    ]
    for copy in small:
        copy.start()

    barrier = pltpu.get_barrier_semaphore()
    beside = (at_z(1), at_z(-1), at_x(1), at_x(-1))
    for device in (*beside, partner):
        pl.semaphore_signal(barrier, inc=1, device_id=device, device_id_type=MESH)

    table[...] = jnp.where(lax.broadcasted_iota(jnp.int32, (16, LANES), 0) < 8, -1.0, 0.0)
    for copy in small[:3]:
        copy.wait()
    table[pl.ds(0, top), pl.ds(0, S)] = routes_ref[...].astype(jnp.float32)
    table[pl.ds(8, top), pl.ds(0, S)] = shares_ref[...]
    tables[0] = table[...].astype(jnp.bfloat16)
    for copy in (*shared_copies(), *expert_copies()):
        copy.start()
    pl.semaphore_wait(barrier, 5)

    for device in beside:
        pl.semaphore_signal(near_sem, inc=1, device_id=device, device_id_type=MESH)

    mixed_copy = send(mixed, mixed_in, m_sem.at[0], m_sem.at[1], partner)
    mixed_copy.start()

    def t_copy(way, k):
        if way == 0:
            return send(tables.at[k], tables.at[k + 1], t_send.at[0, k], t_recv.at[k + 1], at_z(1))
        r = lax.rem(Z - k, Z)
        return send(tables.at[r], tables.at[Z - k - 1], t_send.at[1, k], t_recv.at[Z - k - 1], at_z(-1))

    def t_stage(k):
        for way in (0, 1):
            limit = half - 1

            @pl.when((k >= 1) & (k <= limit))
            def _():
                t_copy(way, k - 1).wait_recv()

            @pl.when(k + 1 <= limit)
            def _():
                t_copy(way, k).start()

    def z_copy(way, k, c):
        if way == 0:
            return send(gathered.at[k, c], gathered.at[k + 1, c], z_send.at[0, k, c], z_recv.at[k + 1, c], at_z(1))
        r = lax.rem(Z - k, Z)
        return send(gathered.at[r, c], gathered.at[Z - k - 1, c], z_send.at[1, k, c], z_recv.at[Z - k - 1, c], at_z(-1))

    def z_stage(k, c):
        for way in (0, 1):
            limit = half - 1

            @pl.when((k >= 1) & (k <= limit))
            def _():
                z_copy(way, k - 1, c).wait_recv()

            @pl.when(k + 1 <= limit)
            def _():
                z_copy(way, k, c).start()

    before = (
        lax.broadcasted_iota(jnp.int32, (LANES, LANES), 0) < lax.broadcasted_iota(jnp.int32, (LANES, LANES), 1)
    ).astype(jnp.float32).astype(jnp.bfloat16)
    offset = lax.broadcasted_iota(jnp.int32, (8, LANES), 0)
    column = offset + x
    column = jnp.where(column >= X, column - X, column)

    def experts_at(dz):
        return jnp.where(offset < X, lax.rem(z + dz + Z, Z) * X + column, -2).astype(jnp.float32)

    def build(r):
        build_for(r, experts_at(0), pick.at[r], spread.at[r])

    def build_for(r, expert_of, pick_ref, spread_ref):
        table = tables[r].astype(jnp.float32)
        named = jnp.zeros((8, LANES), jnp.float32)
        weight = jnp.zeros((8, LANES), jnp.float32)
        for k in range(top):
            hit = table[k : k + 1, :] == expert_of
            named = named + jnp.where(hit, 1.0, 0.0)
            weight = weight + jnp.where(hit, table[8 + k : 9 + k, :], 0.0)
        rank = jnp.dot(named.astype(jnp.bfloat16), before, preferred_element_type=jnp.float32)
        code = jnp.where(named > 0.0, rank, -1.0)
        slot = lax.broadcasted_iota(jnp.int32, (R, LANES), 0).astype(jnp.float32)
        parts, weighted = [], []
        for d in range(X):
            block = jnp.where(code[d : d + 1, :] == slot, 1.0, 0.0)
            parts.append(block)
            weighted.append(block * weight[d : d + 1, :])
        pick_ref[...] = jnp.concatenate(parts, axis=0).astype(jnp.bfloat16)
        spread_ref[...] = jnp.concatenate(weighted, axis=0).T.astype(jnp.bfloat16)

    t_stage(jnp.int32(0))
    build(0)

    for copy in small[3:]:
        copy.wait()
    mixed_copy.wait_recv()
    both = mixed[...].astype(jnp.float32) + mixed_in[...].astype(jnp.float32)
    middle[...] = (tokens_ref[...].astype(jnp.float32) + both).astype(jnp.bfloat16)
    values = middle[...].astype(jnp.float32)
    factor = lax.rsqrt(jnp.mean(values * values, axis=-1, keepdims=True) + norm_eps)

    def own(c):
        return pl.ds(pl.multiple_of(tp * H + c * W, W), W)

    for c in range(nc):
        mine = middle[:, own(c)].astype(jnp.float32) * factor * gain_ref[:, own(c)]
        gathered[0, c] = mine.astype(jnp.bfloat16)
        z_stage(jnp.int32(0), c)
    normed[...] = (values * factor * gain_ref[...]).astype(jnp.bfloat16)

    def shared_hidden():
        for copy in shared_copies():
            copy.wait()
        acc = jnp.dot(normed[...], s_in[...], preferred_element_type=jnp.float32)
        s_hidden[...] = (jax.nn.silu(acc[:, :SF]) * acc[:, SF:]).astype(jnp.bfloat16)

    s_copy = send(s_part.at[other], s_part_in, s_sem.at[0], s_sem.at[1], partner)

    def shared_partial():
        for h in range(2):
            for c in range(nc):
                s_part[h, :, pl.ds(c * W, W)] = jnp.dot(
                    s_hidden[...], s_out[:, pl.ds(h * H + c * W, W)], preferred_element_type=jnp.float32
                ).astype(jnp.bfloat16)
        s_copy.start()

    def x_copy(r, d, c):
        rows = pl.ds(d * R, R)
        return send(staged.at[r, c, rows, :], rows_in.at[r, tp, c, rows, :], x_send.at[r], x_recv.at[r], at_x(d))

    def c_copy(r):
        return send(rows_in.at[r, tp], rows_in.at[r, tp], c_send.at[r], c_recv.at[r], partner)

    def p_copy(r):
        return send(partial.at[r, other], partner_part.at[r], p_send.at[r], p_recv.at[r], partner)

    def b_copy(r, d, c):
        rows = pl.ds(d * R, R)
        return send(total.at[r, c, rows, :], back.at[r, c, rows, :], b_send.at[r], b_recv.at[r, c], at_x(-d))

    def select(r, c):
        chosen = jnp.dot(
            pick[r, :, pl.ds(0, S)], gathered[r, c], preferred_element_type=jnp.float32
        ).astype(jnp.bfloat16)
        rows_in[r, tp, c, pl.ds(0, R), :] = chosen[:R]
        staged[r, c] = chosen
        for d in range(1, X):
            x_copy(r, d, c).start()

    def far_row(way):
        return half - 1 if way == 0 else Z - half + 1

    def far_chunks(way):
        return pl.ds(way * hc, hc)

    def f_copy(way, d, c):
        rows = pl.ds(d * R, R)
        return send(
            far_staged.at[way, c, rows, :],
            rows_in.at[half, tp, way * hc + c, rows, :],
            f_send.at[way],
            x_recv.at[half],
            at_far(1 - 2 * way, d),
        )

    def g_copy(way, d, c):
        rows = pl.ds(d * R, R)
        return send(
            total.at[half, way * hc + c, rows, :],
            far_back.at[way, c, rows, :],
            g_send.at[way],
            f_recv.at[way, c],
            at_far(2 * way - 1, -d),
        )

    def select_far(c):
        way = c // hc
        far_staged[way, c - way * hc] = jnp.dot(
            far_pick[way, :, pl.ds(0, S)], gathered[far_row(way), c], preferred_element_type=jnp.float32
        ).astype(jnp.bfloat16)
        for d in range(X):
            f_copy(way, d, c - way * hc).start()

    def hand_far():
        send(rows_in.at[half, tp], rows_in.at[half, tp], f_send.at[0], x_recv.at[half], partner).wait_recv()
        c_copy(half).start()

    rest = pl.ds(R, (X - 1) * R)

    def hand_over(r):
        send(staged.at[r, :, rest, :], rows_in.at[r, tp, :, rest, :], x_send.at[r], x_recv.at[r], at_x(1)).wait_recv()
        c_copy(r).start()

    def expert(rs):
        M = X * R
        for r in rs:
            send(rows_in.at[r, other], rows_in.at[r, other], c_send.at[r], c_recv.at[r], partner).wait_recv()
        acc = jnp.zeros((len(rs) * M, 2 * F), jnp.float32)
        for h in range(2):
            for c in range(nc):
                rows = jnp.concatenate([rows_in[r, h, c] for r in rs], axis=0)
                acc = acc + jnp.dot(rows, w_in[pl.ds(h * H + c * W, W), :], preferred_element_type=jnp.float32)
        hidden = (jax.nn.silu(acc[:, :F]) * acc[:, F:]).astype(jnp.bfloat16)
        for h in (other, tp):
            for c in range(nc):
                cols = pl.ds(pl.multiple_of(h * H + c * W, W), W)
                piece = jnp.dot(hidden, w_out[:, cols], preferred_element_type=jnp.float32).astype(jnp.bfloat16)
                for n, r in enumerate(rs):
                    partial[r, h, c] = piece[n * M : (n + 1) * M]
            if h is other:
                for r in rs:
                    p_copy(r).start()

    def join(r):
        p_copy(r).wait_recv()
        for c in range(nc):
            join_chunk(r, c)

    def join_chunk(r, c):
        y = (partial[r, tp, c].astype(jnp.float32) + partner_part[r, c].astype(jnp.float32)).astype(jnp.bfloat16)
        back[r, c, pl.ds(0, R), :] = y[:R]
        total[r, c] = y

    def hand_back(r):
        for c in range(nc):
            for d in range(1, X):
                b_copy(r, d, c).start()

    def of_pair(stage, k, way, least=0):
        if way == 0:
            @pl.when((k >= least) & (k < half))
            def _():
                stage(k)
        else:
            @pl.when((k >= 1) & (k < half))
            def _():
                stage(Z - k)

    def step(i, carry):
        @pl.when(i < half)
        def _():
            t_stage(i)

        of_pair(build, i, 0, 1)
        of_pair(build, i, 1, 1)

        @pl.when(i == half - 1)
        def _():
            pl.semaphore_wait(far_sem, 2)
            for way in (0, 1):
                build_for(far_row(way), experts_at(1 - 2 * way), far_pick.at[way], far_spread.at[way])

        for c in range(nc):
            z_stage(i, c)

            @pl.when(i == half - 1)
            def _():
                select_far(c)

            of_pair(functools.partial(select, c=c), i, 0, 1)
            of_pair(functools.partial(select, c=c), i, 1, 1)
            if c == 1:

                @pl.when(i == 2)
                def _():
                    for copy in expert_copies():
                        copy.wait()
                    expert([0])

                @pl.when(i > 2)
                def _():
                    expert([i - 2, Z - i + 2])

            if c == 2:
                of_pair(join, i - 3, 0)
                of_pair(join, i - 3, 1)

        @pl.when(i == half)
        def _():
            hand_far()

        of_pair(hand_over, i - 1, 0)
        of_pair(hand_over, i - 1, 1)
        return carry

    pl.semaphore_wait(near_sem, 4)
    for device in beside[:2]:
        pl.semaphore_signal(far_sem, inc=1, device_id=device, device_id_type=MESH)
    for c in range(nc):
        select(0, c)
    lax.fori_loop(1, half + 1, step, 0)

    last = (half - 1, half + 1, half)
    expert(last)
    join(half - 2)
    if half > 2:
        join(half + 2)
    for r in last:
        p_copy(r).wait_recv()
    for c in range(nc):
        for r in last:
            join_chunk(r, c)
        for d in range(X):
            g_copy(c // hc, d, c - c // hc * hc).start()
        for d in range(1, X):
            b_copy(half - 1, d, c).start()
            b_copy(half + 1, d, c).start()
    hand_back(half - 2)
    if half > 2:
        hand_back(half + 2)
    shared_hidden()
    shared_partial()

    def r_copy(way, k, c):
        if way == 0:
            return send(sums_out.at[k, c], sums_in.at[k - 1, c], r_send.at[k, c], r_recv.at[k - 1, c], at_z(-1))
        return send(sums_out.at[Z - k, c], sums_in.at[Z - k + 1, c], r_send.at[Z - k, c], r_recv.at[Z - k + 1, c], at_z(1))

    def share_of(r, c):
        return jnp.dot(spread[r, pl.ds(0, S), :], back[r, c], preferred_element_type=jnp.float32)

    def back_wait(r, c):
        send(total.at[r, c, rest, :], back.at[r, c, rest, :], b_send.at[r], b_recv.at[r, c], at_x(1)).wait_recv()

    def go_back(i, carry):
        k = half - 1 - i
        of_pair(hand_back, k - 2, 0)
        of_pair(hand_back, k - 2, 1)
        for c in range(nc):
            back_wait(k, c)
            back_wait(Z - k, c)

            @pl.when(k == half - 1)
            def _():
                way, at = c // hc, c - c // hc * hc
                send(
                    far_staged.at[way, at], far_back.at[way, at], g_send.at[way], f_recv.at[way, at], partner
                ).wait_recv()

            for way in (0, 1):
                r = k if way == 0 else Z - k
                mine = share_of(r, c)

                @pl.when(k == half - 1)
                def _():
                    first = mine
                    if c // hc == way:
                        first = mine + jnp.dot(
                            far_spread[way, pl.ds(0, S), :],
                            far_back[way, c - way * hc],
                            preferred_element_type=jnp.float32,
                        )
                    sums_out[r, c] = first.astype(jnp.bfloat16)

                @pl.when(k < half - 1)
                def _():
                    r_copy(way, k + 1, c).wait_recv()
                    sums_out[r, c] = (mine + sums_in[r, c].astype(jnp.float32)).astype(jnp.bfloat16)

                r_copy(way, k, c).start()
        return carry

    lax.fori_loop(0, half - 1, go_back, 0)

    for c in range(nc):
        back_wait(0, c)
    s_copy.wait_recv()
    for c in range(nc):
        mine = share_of(0, c) + middle[:, own(c)].astype(jnp.float32)
        mine = mine + s_part[tp, :, pl.ds(c * W, W)].astype(jnp.float32)
        mine = mine + s_part_in[:, pl.ds(c * W, W)].astype(jnp.float32)
        r_copy(0, 1, c).wait_recv()
        r_copy(1, 1, c).wait_recv()
        mine = mine + sums_in[0, c].astype(jnp.float32) + sums_in[Z, c].astype(jnp.float32)
        out_ref[:, pl.ds(c * W, W)] = mine.astype(out_ref.dtype)

    mixed_copy.wait_send()
    s_copy.wait_send()

    def drain(k, carry):
        for way in (0, 1):
            t_copy(way, k).wait_send()
            for c in range(nc):
                z_copy(way, k, c).wait_send()
                r_copy(way, k + 1, c).wait_send()
        return carry

    lax.fori_loop(0, half - 1, drain, 0)

    def drain_rows(r, carry):
        @pl.when(r != half)
        def _():
            send(staged.at[r, :, rest, :], rows_in.at[r, tp, :, rest, :], x_send.at[r], x_recv.at[r], at_x(1)).wait_send()
            send(total.at[r, :, rest, :], back.at[r, :, rest, :], b_send.at[r], b_recv.at[r, 0], at_x(1)).wait_send()

        c_copy(r).wait_send()
        p_copy(r).wait_send()
        return carry

    lax.fori_loop(0, Z, drain_rows, 0)
    for way in (0, 1):
        send(far_staged.at[way], far_back.at[way], f_send.at[way], f_recv.at[way, 0], partner).wait_send()
        send(total.at[half, far_chunks(way)], far_back.at[way], g_send.at[way], f_recv.at[way, 0], partner).wait_send()


def layer(mixed, tokens, gain, routes, shares, sgate, sup, sdown, gate, up, down):
    top = routes.shape[1]
    S, D = tokens.shape
    H = D // lax.axis_size("tp")
    X = ROW_RING
    Z = lax.axis_size("ep") // X
    nc = CHUNKS
    W = H // nc
    R = 16
    F = gate.shape[2]
    SF = sgate.shape[1]
    bf = jnp.bfloat16
    dma = pltpu.SemaphoreType.DMA
    vm = pl.BlockSpec(memory_space=pltpu.VMEM)
    hb = pl.BlockSpec(memory_space=pl.ANY)
    return pl.pallas_call(
        functools.partial(layer_kernel, (Z, X, S, H, R, nc, top)),
        out_shape=jax.ShapeDtypeStruct((S, H), bf),
        in_specs=[hb] * 11,
        out_specs=vm,
        scratch_shapes=[
            pltpu.VMEM((S, D), bf),
            pltpu.VMEM((1, D), jnp.float32),
            pltpu.VMEM((top, S), jnp.int32),
            pltpu.VMEM((top, S), jnp.float32),
            pltpu.VMEM((16, LANES), jnp.float32),
            pltpu.VMEM((S, D), bf),
            pltpu.VMEM((S, D), bf),
            pltpu.VMEM((S, D), bf),
            pltpu.VMEM((S, D), bf),
            pltpu.VMEM((D, 2 * SF), bf),
            pltpu.VMEM((SF, D), bf),
            pltpu.VMEM((S, SF), bf),
            pltpu.VMEM((2, S, H), bf),
            pltpu.VMEM((S, H), bf),
            pltpu.VMEM((Z, nc, S, W), bf),
            pltpu.VMEM((Z, 16, LANES), bf),
            pltpu.VMEM((Z, X * R, LANES), bf),
            pltpu.VMEM((Z, LANES, X * R), bf),
            pltpu.VMEM((Z, nc, X * R, W), bf),
            pltpu.VMEM((Z, 2, nc, X * R, W), bf),
            pltpu.VMEM((D, 2 * F), bf),
            pltpu.VMEM((F, D), bf),
            pltpu.VMEM((Z, 2, nc, X * R, W), bf),
            pltpu.VMEM((Z, nc, X * R, W), bf),
            pltpu.VMEM((Z, nc, X * R, W), bf),
            pltpu.VMEM((Z, nc, X * R, W), bf),
            pltpu.VMEM((Z + 1, nc, S, W), bf),
            pltpu.VMEM((Z, nc, S, W), bf),
            pltpu.VMEM((2, X * R, LANES), bf),
            pltpu.VMEM((2, LANES, X * R), bf),
            pltpu.VMEM((2, nc // 2, X * R, W), bf),
            pltpu.VMEM((2, nc // 2, X * R, W), bf),
            dma((12,)),
            dma((2,)),
            dma((2,)),
            dma((2, Z // 2)),
            dma((Z,)),
            dma((2, Z // 2, nc)),
            dma((Z, nc)),
            dma((Z,)),
            dma((Z,)),
            dma((Z,)),
            dma((Z,)),
            dma((Z,)),
            dma((Z,)),
            dma((Z,)),
            dma((Z, nc)),
            dma((Z, nc)),
            dma((Z + 1, nc)),
            dma((2,)),
            dma((2, nc // 2)),
            dma((2,)),
            pltpu.SemaphoreType.REGULAR,
            pltpu.SemaphoreType.REGULAR,
        ],
        compiler_params=pltpu.CompilerParams(
            collective_id=0, has_side_effects=True, vmem_limit_bytes=56300000
        ),
        name="layer",
    )(mixed, tokens, gain[None, :], routes.T, shares.T, sgate, sup, sdown, gate, up, down)


def mixer_kernel(
    tokens_hbm,
    prior_hbm,
    gain_hbm,
    weight_hbm,
    decay_hbm,
    freq_hbm,
    step_hbm,
    imap_hbm,
    omap_hbm,
    skip_hbm,
    project_hbm,
    mixed_hbm,
    state_hbm,
    tokens_ref,
    old,
    gain_ref,
    weight,
    decay_ref,
    freq_ref,
    step_ref,
    imap_ref,
    omap_ref,
    skip_ref,
    project,
    active_ref,
    mixed,
    fresh,
    in_sem,
    out_sem,
    mixed_sem,
):
    S, D = tokens_ref.shape
    width = weight.shape[1]
    groups, entries = decay_ref.shape
    members = width // groups
    f4, bf = jnp.float32, jnp.bfloat16
    lane_groups = LANES // entries
    block = LANES // members
    cols = block * entries

    fetched = {}
    for i, (name, src, dst) in enumerate(
        (
            ("tokens", tokens_hbm, tokens_ref),
            ("gain", gain_hbm, gain_ref),
            ("step", step_hbm, step_ref),
            ("decay", decay_hbm, decay_ref),
            ("freq", freq_hbm, freq_ref),
            ("weight", weight_hbm, weight),
            ("imap", imap_hbm, imap_ref),
            ("old", prior_hbm, old),
            ("skip", skip_hbm, skip_ref),
            ("omap", omap_hbm, omap_ref),
            ("project", project_hbm, project),
        )
    ):
        fetched[name] = pltpu.make_async_copy(src, dst, in_sem.at[i])
        fetched[name].start()

    def state_copy(part, q):
        lanes = pl.ds(q * cols, cols)
        return pltpu.make_async_copy(fresh.at[part, :, lanes], state_hbm.at[part, :, lanes], out_sem.at[part, q])

    for name in ("step", "decay", "freq"):
        fetched[name].wait()

    eye = lax.broadcasted_iota(jnp.int32, (groups, groups), 0) == lax.broadcasted_iota(jnp.int32, (groups, groups), 1)
    log_column = jnp.sum(jnp.where(eye, step_ref[...], 0.0), axis=1, keepdims=True)
    step_size = jnp.exp(log_column)
    real_rate = -decay_ref[...]
    frequency = freq_ref[...]
    magnitude = jnp.exp(real_rate * step_size)
    turn_real = magnitude * jnp.cos(frequency * step_size)
    turn_imag = magnitude * jnp.sin(frequency * step_size)
    denominator = real_rate * real_rate + frequency * frequency
    hold_real = ((turn_real - 1.0) * real_rate + turn_imag * frequency) / denominator
    hold_imag = (turn_imag * real_rate - (turn_real - 1.0) * frequency) / denominator
    doubled = [jnp.concatenate([v] * lane_groups, axis=1) for v in (turn_real, turn_imag, hold_real, hold_imag)]
    row_group = lax.broadcasted_iota(jnp.int32, (groups, LANES), 0)
    lane_group = lax.broadcasted_iota(jnp.int32, (groups, LANES), 1) // entries

    fetched["tokens"].wait()
    fetched["gain"].wait()
    values = tokens_ref[...].astype(f4)
    factor = lax.rsqrt(jnp.mean(values * values, axis=-1, keepdims=True) + norm_eps)
    normed = (values * factor * gain_ref[...]).astype(bf)
    fetched["weight"].wait()
    drive = jnp.dot(normed, weight[...], preferred_element_type=f4).astype(bf)
    for name in ("imap", "old", "skip", "omap"):
        fetched[name].wait()

    in_row = lax.broadcasted_iota(jnp.int32, (LANES, LANES), 0) // members
    in_lane = lax.broadcasted_iota(jnp.int32, (LANES, LANES), 1) // entries
    out_row = lax.broadcasted_iota(jnp.int32, (LANES, 2 * LANES), 0) // members
    out_lane = lax.broadcasted_iota(jnp.int32, (LANES, 2 * LANES), 1) // entries

    for q in range(width // LANES):
        channels = slice(q * LANES, (q + 1) * LANES)
        mine = drive[:, channels]
        maps = [jnp.concatenate([imap_ref[part, channels, :]] * lane_groups, axis=1) for part in range(2)]
        outs = [jnp.concatenate([omap_ref[part, channels, :]] * (2 * lane_groups), axis=1) for part in range(2)]
        readout = mine.astype(f4) * skip_ref[:, channels]
        for m in range(cols // LANES):
            mask = in_row == in_lane + m * lane_groups
            both = jnp.concatenate([jnp.where(mask, v, 0.0) for v in maps], axis=1).astype(bf)
            push = jnp.dot(mine, both, preferred_element_type=f4)
            push_real, push_imag = push[:, :LANES], push[:, LANES:]
            first = q * block + m * lane_groups
            tr, ti, hr, hi = [
                jnp.sum(jnp.where(row_group == lane_group + first, v, 0.0), axis=0, keepdims=True) for v in doubled
            ]
            at = slice(q * cols + m * LANES, q * cols + (m + 1) * LANES)
            old_real, old_imag = old[0, :, at], old[1, :, at]
            fresh[0, :, at] = tr * old_real - ti * old_imag + (push_real * hr - push_imag * hi)
            fresh[1, :, at] = tr * old_imag + ti * old_real + (push_real * hi + push_imag * hr)
        state_copy(0, q).start()
        state_copy(1, q).start()
        for h in range(cols // (2 * LANES)):
            at = slice(q * cols + h * 2 * LANES, q * cols + (h + 1) * 2 * LANES)
            mask = out_row == out_lane + h * 2 * lane_groups
            for part in range(2):
                spread_out = jnp.where(mask, outs[part] if part == 0 else -outs[part], 0.0).astype(bf)
                readout = readout + lax.dot_general(
                    fresh[part, :, at].astype(bf), spread_out, (((1,), (1,)), ((), ())), preferred_element_type=f4
                )
        active_ref[:, channels] = jax.nn.gelu(readout).astype(bf)
    fetched["project"].wait()
    quarter = D // 4
    sent = []
    for h in range(4):
        at = slice(h * quarter, (h + 1) * quarter)
        mixed[:, at] = jnp.dot(active_ref[...], project[:, at], preferred_element_type=f4).astype(bf)
        sent.append(pltpu.make_async_copy(mixed.at[:, at], mixed_hbm.at[:, at], mixed_sem.at[h]))
        sent[-1].start()
    for copy in sent:
        copy.wait()
    for q in range(width // LANES):
        for part in range(2):
            state_copy(part, q).wait()


def mixer(tokens, prior, gain, weight, decay, freq, log_step, imap, omap, skip, project):
    S, D = tokens.shape
    width = weight.shape[1]
    f4 = jnp.float32
    hb = pl.BlockSpec(memory_space=pl.ANY)
    dma = pltpu.SemaphoreType.DMA
    by_channel = (2, width, imap.shape[2])
    return pl.pallas_call(
        mixer_kernel,
        out_shape=(
            jax.ShapeDtypeStruct((S, D), jnp.bfloat16),
            jax.ShapeDtypeStruct(prior.shape, jnp.float32),
        ),
        in_specs=[hb] * 11,
        out_specs=(hb, hb),
        scratch_shapes=[
            pltpu.VMEM((S, D), tokens.dtype),
            pltpu.VMEM(prior.shape, f4),
            pltpu.VMEM((1, D), f4),
            pltpu.VMEM(weight.shape, weight.dtype),
            pltpu.VMEM(decay.shape, f4),
            pltpu.VMEM(freq.shape, f4),
            pltpu.VMEM((1, log_step.shape[0]), f4),
            pltpu.VMEM(by_channel, f4),
            pltpu.VMEM(by_channel, f4),
            pltpu.VMEM((1, width), f4),
            pltpu.VMEM(project.shape, project.dtype),
            pltpu.VMEM((S, width), tokens.dtype),
            pltpu.VMEM((S, D), tokens.dtype),
            pltpu.VMEM(prior.shape, f4),
            dma((11,)),
            dma((2, width // LANES)),
            dma((4,)),
        ],
        compiler_params=pltpu.CompilerParams(vmem_limit_bytes=VMEM_ALL),
        name="mixer",
    )(
        tokens,
        prior,
        gain[None, :],
        weight,
        decay,
        freq,
        log_step[None, :],
        jnp.swapaxes(imap, 2, 3).reshape(by_channel),
        omap.reshape(by_channel),
        skip[None, :],
        project,
    )


def body(
    tokens,
    prior_state,
    mix_gain,
    in_weight,
    decay_rate,
    frequency,
    log_step,
    input_map,
    output_map,
    skip_gain,
    out_weight,
    channel_gain,
    expert_gate,
    expert_up,
    expert_down,
    shared_gate,
    shared_up,
    shared_down,
    routes,
    route_weights,
):
    mixed, new_state = mixer(
        tokens,
        prior_state,
        mix_gain,
        in_weight,
        decay_rate,
        frequency,
        log_step,
        input_map,
        output_map,
        skip_gain,
        out_weight,
    )
    layer_out = layer(
        mixed,
        tokens,
        channel_gain,
        routes,
        route_weights,
        shared_gate,
        shared_up,
        shared_down,
        expert_gate,
        expert_up,
        expert_down,
    )
    return (layer_out, new_state)


def solution(mesh):
    in_specs = (
        P(("grp", "ep"), None),
        P(None, ("grp", "ep"), "tp"),
        P(),
        P(None, "tp"),
        P("tp", None),
        P("tp", None),
        P("tp"),
        P(None, "tp", None, None),
        P(None, "tp", None, None),
        P("tp"),
        P("tp", None),
        P(),
        P("ep", None, "tp"),
        P("ep", None, "tp"),
        P("ep", "tp", None),
        P(None, "tp"),
        P(None, "tp"),
        P("tp", None),
        P(("grp", "ep"), None),
        P(("grp", "ep"), None),
    )
    out_specs = (P(("grp", "ep"), "tp"), P(None, ("grp", "ep"), "tp"))
    return jax.shard_map(body, mesh=mesh, in_specs=in_specs, out_specs=out_specs, check_vma=False)
```

```python
import functools

import jax
import jax.numpy as jnp
from jax import lax
from jax.experimental import pallas as pl
from jax.experimental.pallas import tpu as pltpu
from jax.sharding import PartitionSpec as P

MESH = pl.DeviceIdType.MESH
norm_eps = 1e-06
ROW_RING = 4
CHUNKS = 4
LANES = 128
VMEM_ALL = 63 * 1024 * 1024


def layer_kernel(
    cfg,
    mixed_hbm,
    tokens_hbm,
    gain_hbm,
    routes_hbm,
    shares_hbm,
    sgate_hbm,
    sup_hbm,
    sdown_hbm,
    gate_hbm,
    up_hbm,
    down_hbm,
    out_ref,
    tokens_ref,
    gain_ref,
    routes_ref,
    shares_ref,
    table,
    mixed,
    mixed_in,
    middle,
    normed,
    s_in,
    s_out,
    s_hidden,
    s_part,
    s_part_in,
    gathered,
    tables,
    pick,
    spread,
    staged,
    rows_in,
    w_in,
    w_out,
    partial,
    partner_part,
    total,
    back,
    sums_in,
    sums_out,
    far_pick,
    far_spread,
    far_staged,
    far_back,
    w_sem,
    m_sem,
    s_sem,
    t_send,
    t_recv,
    z_send,
    z_recv,
    x_send,
    x_recv,
    c_send,
    c_recv,
    p_send,
    p_recv,
    b_send,
    b_recv,
    r_send,
    r_recv,
    f_send,
    f_recv,
    g_send,
    near_sem,
    far_sem,
):
    Z, X, S, H, R, nc, top = cfg
    W = H // nc
    half = Z // 2
    F = gate_hbm.shape[2]
    SF = sgate_hbm.shape[1]
    ep = lax.axis_index("ep")
    tp = lax.axis_index("tp")
    other = 1 - tp
    z, x = ep // X, lax.rem(ep, X)

    def at_z(offset):
        return {"ep": lax.rem(z + offset + Z, Z) * X + x}

    def at_x(offset):
        return {"ep": z * X + lax.rem(x + offset + X, X)}

    def at_far(dz, dx):
        return {"ep": lax.rem(z + dz + Z, Z) * X + lax.rem(x + dx + X, X)}

    partner = {"tp": other}
    hc = nc // 2

    def send(src, dst, s_sem, r_sem, device):
        return pltpu.make_async_remote_copy(
            src_ref=src, dst_ref=dst, send_sem=s_sem, recv_sem=r_sem,
            device_id=device, device_id_type=MESH,
        )

    def shared_copies():
        return (
            pltpu.make_async_copy(sgate_hbm, s_in.at[:, pl.ds(0, SF)], w_sem.at[1]),
            pltpu.make_async_copy(sup_hbm, s_in.at[:, pl.ds(SF, SF)], w_sem.at[2]),
            pltpu.make_async_copy(sdown_hbm, s_out, w_sem.at[3]),
        )

    def expert_copies():
        return (
            pltpu.make_async_copy(gate_hbm.at[0], w_in.at[:, pl.ds(0, F)], w_sem.at[4]),
            pltpu.make_async_copy(up_hbm.at[0], w_in.at[:, pl.ds(F, F)], w_sem.at[5]),
            pltpu.make_async_copy(down_hbm.at[0], w_out, w_sem.at[6]),
        )

    small = [
        pltpu.make_async_copy(src, dst, w_sem.at[7 + i])
        for i, (src, dst) in enumerate(
            (
                (mixed_hbm, mixed),
                (routes_hbm, routes_ref),
                (shares_hbm, shares_ref),
                (tokens_hbm, tokens_ref),
                (gain_hbm, gain_ref),
            )
        )
    ]
    for copy in small:
        copy.start()

    barrier = pltpu.get_barrier_semaphore()
    beside = (at_z(1), at_z(-1), at_x(1), at_x(-1))
    for device in (*beside, partner):
        pl.semaphore_signal(barrier, inc=1, device_id=device, device_id_type=MESH)

    table[...] = jnp.where(lax.broadcasted_iota(jnp.int32, (16, LANES), 0) < 8, -1.0, 0.0)
    for copy in small[:3]:
        copy.wait()
    table[pl.ds(0, top), pl.ds(0, S)] = routes_ref[...].astype(jnp.float32)
    table[pl.ds(8, top), pl.ds(0, S)] = shares_ref[...]
    tables[0] = table[...].astype(jnp.bfloat16)
    for copy in (*shared_copies(), *expert_copies()):
        copy.start()
    pl.semaphore_wait(barrier, 5)

    for device in beside:
        pl.semaphore_signal(near_sem, inc=1, device_id=device, device_id_type=MESH)

    mixed_copy = send(mixed, mixed_in, m_sem.at[0], m_sem.at[1], partner)
    mixed_copy.start()

    def t_copy(way, k):
        if way == 0:
            return send(tables.at[k], tables.at[k + 1], t_send.at[0, k], t_recv.at[k + 1], at_z(1))
        r = lax.rem(Z - k, Z)
        return send(tables.at[r], tables.at[Z - k - 1], t_send.at[1, k], t_recv.at[Z - k - 1], at_z(-1))

    def t_stage(k):
        for way in (0, 1):
            limit = half - 1

            @pl.when((k >= 1) & (k <= limit))
            def _():
                t_copy(way, k - 1).wait_recv()

            @pl.when(k + 1 <= limit)
            def _():
                t_copy(way, k).start()

    def z_copy(way, k, c):
        if way == 0:
            return send(gathered.at[k, c], gathered.at[k + 1, c], z_send.at[0, k, c], z_recv.at[k + 1, c], at_z(1))
        r = lax.rem(Z - k, Z)
        return send(gathered.at[r, c], gathered.at[Z - k - 1, c], z_send.at[1, k, c], z_recv.at[Z - k - 1, c], at_z(-1))

    def z_stage(k, c):
        for way in (0, 1):
            limit = half - 1

            @pl.when((k >= 1) & (k <= limit))
            def _():
                z_copy(way, k - 1, c).wait_recv()

            @pl.when(k + 1 <= limit)
            def _():
                z_copy(way, k, c).start()

    before = (
        lax.broadcasted_iota(jnp.int32, (LANES, LANES), 0) < lax.broadcasted_iota(jnp.int32, (LANES, LANES), 1)
    ).astype(jnp.float32).astype(jnp.bfloat16)
    offset = lax.broadcasted_iota(jnp.int32, (8, LANES), 0)
    column = offset + x
    column = jnp.where(column >= X, column - X, column)

    def experts_at(dz):
        return jnp.where(offset < X, lax.rem(z + dz + Z, Z) * X + column, -2).astype(jnp.float32)

    def build(r):
        build_for(r, experts_at(0), pick.at[r], spread.at[r])

    def build_for(r, expert_of, pick_ref, spread_ref):
        table = tables[r].astype(jnp.float32)
        named = jnp.zeros((8, LANES), jnp.float32)
        weight = jnp.zeros((8, LANES), jnp.float32)
        for k in range(top):
            hit = table[k : k + 1, :] == expert_of
            named = named + jnp.where(hit, 1.0, 0.0)
            weight = weight + jnp.where(hit, table[8 + k : 9 + k, :], 0.0)
        rank = jnp.dot(named.astype(jnp.bfloat16), before, preferred_element_type=jnp.float32)
        code = jnp.where(named > 0.0, rank, -1.0)
        slot = lax.broadcasted_iota(jnp.int32, (R, LANES), 0).astype(jnp.float32)
        parts, weighted = [], []
        for d in range(X):
            block = jnp.where(code[d : d + 1, :] == slot, 1.0, 0.0)
            parts.append(block)
            weighted.append(block * weight[d : d + 1, :])
        pick_ref[...] = jnp.concatenate(parts, axis=0).astype(jnp.bfloat16)
        spread_ref[...] = jnp.concatenate(weighted, axis=0).T.astype(jnp.bfloat16)

    t_stage(jnp.int32(0))
    build(0)

    for copy in small[3:]:
        copy.wait()
    mixed_copy.wait_recv()
    both = mixed[...].astype(jnp.float32) + mixed_in[...].astype(jnp.float32)
    middle[...] = (tokens_ref[...].astype(jnp.float32) + both).astype(jnp.bfloat16)
    values = middle[...].astype(jnp.float32)
    factor = lax.rsqrt(jnp.mean(values * values, axis=-1, keepdims=True) + norm_eps)

    def own(c):
        return pl.ds(pl.multiple_of(tp * H + c * W, W), W)

    for c in range(nc):
        mine = middle[:, own(c)].astype(jnp.float32) * factor * gain_ref[:, own(c)]
        gathered[0, c] = mine.astype(jnp.bfloat16)
        z_stage(jnp.int32(0), c)
    normed[...] = (values * factor * gain_ref[...]).astype(jnp.bfloat16)

    def shared_hidden():
        for copy in shared_copies():
            copy.wait()
        acc = jnp.dot(normed[...], s_in[...], preferred_element_type=jnp.float32)
        s_hidden[...] = (jax.nn.silu(acc[:, :SF]) * acc[:, SF:]).astype(jnp.bfloat16)

    s_copy = send(s_part.at[other], s_part_in, s_sem.at[0], s_sem.at[1], partner)

    def shared_partial():
        for h in range(2):
            for c in range(nc):
                s_part[h, :, pl.ds(c * W, W)] = jnp.dot(
                    s_hidden[...], s_out[:, pl.ds(h * H + c * W, W)], preferred_element_type=jnp.float32
                ).astype(jnp.bfloat16)
        s_copy.start()

    def x_copy(r, d, c):
        rows = pl.ds(d * R, R)
        return send(staged.at[r, c, rows, :], rows_in.at[r, tp, c, rows, :], x_send.at[r], x_recv.at[r], at_x(d))

    def c_copy(r):
        return send(rows_in.at[r, tp], rows_in.at[r, tp], c_send.at[r], c_recv.at[r], partner)

    def p_copy(r):
        return send(partial.at[r, other], partner_part.at[r], p_send.at[r], p_recv.at[r], partner)

    def b_copy(r, d, c):
        rows = pl.ds(d * R, R)
        return send(total.at[r, c, rows, :], back.at[r, c, rows, :], b_send.at[r], b_recv.at[r, c], at_x(-d))

    def select(r, c):
        chosen = jnp.dot(
            pick[r, :, pl.ds(0, S)], gathered[r, c], preferred_element_type=jnp.float32
        ).astype(jnp.bfloat16)
        rows_in[r, tp, c, pl.ds(0, R), :] = chosen[:R]
        staged[r, c] = chosen
        for d in range(1, X):
            x_copy(r, d, c).start()

    def far_row(way):
        return half - 1 if way == 0 else Z - half + 1

    def far_chunks(way):
        return pl.ds(way * hc, hc)

    def f_copy(way, d, c):
        rows = pl.ds(d * R, R)
        return send(
            far_staged.at[way, c, rows, :],
            rows_in.at[half, tp, way * hc + c, rows, :],
            f_send.at[way],
            x_recv.at[half],
            at_far(1 - 2 * way, d),
        )

    def g_copy(way, d, c):
        rows = pl.ds(d * R, R)
        return send(
            total.at[half, way * hc + c, rows, :],
            far_back.at[way, c, rows, :],
            g_send.at[way],
            f_recv.at[way, c],
            at_far(2 * way - 1, -d),
        )

    def select_far(c):
        way = c // hc
        far_staged[way, c - way * hc] = jnp.dot(
            far_pick[way, :, pl.ds(0, S)], gathered[far_row(way), c], preferred_element_type=jnp.float32
        ).astype(jnp.bfloat16)
        for d in range(X):
            f_copy(way, d, c - way * hc).start()

    def hand_far():
        send(rows_in.at[half, tp], rows_in.at[half, tp], f_send.at[0], x_recv.at[half], partner).wait_recv()
        c_copy(half).start()

    rest = pl.ds(R, (X - 1) * R)

    def hand_over(r):
        send(staged.at[r, :, rest, :], rows_in.at[r, tp, :, rest, :], x_send.at[r], x_recv.at[r], at_x(1)).wait_recv()
        c_copy(r).start()

    def expert(rs):
        M = X * R
        acc = jnp.zeros((len(rs) * M, 2 * F), jnp.float32)
        for h in (tp, other):
            if h is other:
                for r in rs:
                    send(rows_in.at[r, other], rows_in.at[r, other], c_send.at[r], c_recv.at[r], partner).wait_recv()
            for c in range(nc):
                rows = jnp.concatenate([rows_in[r, h, c] for r in rs], axis=0)
                depth = pl.ds(pl.multiple_of(h * H + c * W, W), W)
                acc = acc + jnp.dot(rows, w_in[depth, :], preferred_element_type=jnp.float32)
        hidden = (jax.nn.silu(acc[:, :F]) * acc[:, F:]).astype(jnp.bfloat16)
        for h in (other, tp):
            for c in range(nc):
                cols = pl.ds(pl.multiple_of(h * H + c * W, W), W)
                piece = jnp.dot(hidden, w_out[:, cols], preferred_element_type=jnp.float32).astype(jnp.bfloat16)
                for n, r in enumerate(rs):
                    partial[r, h, c] = piece[n * M : (n + 1) * M]
            if h is other:
                for r in rs:
                    p_copy(r).start()

    def join(r):
        p_copy(r).wait_recv()
        for c in range(nc):
            join_chunk(r, c)

    def join_chunk(r, c):
        y = (partial[r, tp, c].astype(jnp.float32) + partner_part[r, c].astype(jnp.float32)).astype(jnp.bfloat16)
        back[r, c, pl.ds(0, R), :] = y[:R]
        total[r, c] = y

    def hand_back(r):
        for c in range(nc):
            for d in range(1, X):
                b_copy(r, d, c).start()

    def of_pair(stage, k, way, least=0):
        if way == 0:
            @pl.when((k >= least) & (k < half))
            def _():
                stage(k)
        else:
            @pl.when((k >= 1) & (k < half))
            def _():
                stage(Z - k)

    def step(i, carry):
        @pl.when(i < half)
        def _():
            t_stage(i)

        of_pair(build, i, 0, 1)
        of_pair(build, i, 1, 1)

        @pl.when(i == half - 1)
        def _():
            pl.semaphore_wait(far_sem, 2)
            for way in (0, 1):
                build_for(far_row(way), experts_at(1 - 2 * way), far_pick.at[way], far_spread.at[way])

        for c in range(nc):
            z_stage(i, c)

            @pl.when(i == half - 1)
            def _():
                select_far(c)

            of_pair(functools.partial(select, c=c), i, 0, 1)
            of_pair(functools.partial(select, c=c), i, 1, 1)
            if c == 1:

                @pl.when(i == 2)
                def _():
                    for copy in expert_copies():
                        copy.wait()
                    expert([0])

                @pl.when(i > 2)
                def _():
                    expert([i - 2, Z - i + 2])

            if c == 2:
                of_pair(join, i - 3, 0)
                of_pair(join, i - 3, 1)

        @pl.when(i == half)
        def _():
            hand_far()

        of_pair(hand_over, i - 1, 0)
        of_pair(hand_over, i - 1, 1)
        return carry

    pl.semaphore_wait(near_sem, 4)
    for device in beside[:2]:
        pl.semaphore_signal(far_sem, inc=1, device_id=device, device_id_type=MESH)
    for c in range(nc):
        select(0, c)
    lax.fori_loop(1, half + 1, step, 0)

    last = (half - 1, half + 1, half)
    expert(last)
    join(half - 2)
    if half > 2:
        join(half + 2)
    for r in last:
        p_copy(r).wait_recv()
    for c in range(nc):
        for r in last:
            join_chunk(r, c)
        for d in range(X):
            g_copy(c // hc, d, c - c // hc * hc).start()
        for d in range(1, X):
            b_copy(half - 1, d, c).start()
            b_copy(half + 1, d, c).start()
    hand_back(half - 2)
    if half > 2:
        hand_back(half + 2)
    shared_hidden()
    shared_partial()

    def r_copy(way, k, c):
        if way == 0:
            return send(sums_out.at[k, c], sums_in.at[k - 1, c], r_send.at[k, c], r_recv.at[k - 1, c], at_z(-1))
        return send(sums_out.at[Z - k, c], sums_in.at[Z - k + 1, c], r_send.at[Z - k, c], r_recv.at[Z - k + 1, c], at_z(1))

    def share_of(r, c):
        return jnp.dot(spread[r, pl.ds(0, S), :], back[r, c], preferred_element_type=jnp.float32)

    def back_wait(r, c):
        send(total.at[r, c, rest, :], back.at[r, c, rest, :], b_send.at[r], b_recv.at[r, c], at_x(1)).wait_recv()

    def go_back(i, carry):
        k = half - 1 - i
        of_pair(hand_back, k - 2, 0)
        of_pair(hand_back, k - 2, 1)
        for c in range(nc):
            back_wait(k, c)
            back_wait(Z - k, c)

            @pl.when(k == half - 1)
            def _():
                way, at = c // hc, c - c // hc * hc
                send(
                    far_staged.at[way, at], far_back.at[way, at], g_send.at[way], f_recv.at[way, at], partner
                ).wait_recv()

            for way in (0, 1):
                r = k if way == 0 else Z - k
                mine = share_of(r, c)

                @pl.when(k == half - 1)
                def _():
                    first = mine
                    if c // hc == way:
                        first = mine + jnp.dot(
                            far_spread[way, pl.ds(0, S), :],
                            far_back[way, c - way * hc],
                            preferred_element_type=jnp.float32,
                        )
                    sums_out[r, c] = first.astype(jnp.bfloat16)

                @pl.when(k < half - 1)
                def _():
                    r_copy(way, k + 1, c).wait_recv()
                    sums_out[r, c] = (mine + sums_in[r, c].astype(jnp.float32)).astype(jnp.bfloat16)

                r_copy(way, k, c).start()
        return carry

    lax.fori_loop(0, half - 1, go_back, 0)

    for c in range(nc):
        back_wait(0, c)
    s_copy.wait_recv()
    for c in range(nc):
        mine = share_of(0, c) + middle[:, own(c)].astype(jnp.float32)
        mine = mine + s_part[tp, :, pl.ds(c * W, W)].astype(jnp.float32)
        mine = mine + s_part_in[:, pl.ds(c * W, W)].astype(jnp.float32)
        r_copy(0, 1, c).wait_recv()
        r_copy(1, 1, c).wait_recv()
        mine = mine + sums_in[0, c].astype(jnp.float32) + sums_in[Z, c].astype(jnp.float32)
        out_ref[:, pl.ds(c * W, W)] = mine.astype(out_ref.dtype)

    mixed_copy.wait_send()
    s_copy.wait_send()

    def drain(k, carry):
        for way in (0, 1):
            t_copy(way, k).wait_send()
            for c in range(nc):
                z_copy(way, k, c).wait_send()
                r_copy(way, k + 1, c).wait_send()
        return carry

    lax.fori_loop(0, half - 1, drain, 0)

    def drain_rows(r, carry):
        @pl.when(r != half)
        def _():
            send(staged.at[r, :, rest, :], rows_in.at[r, tp, :, rest, :], x_send.at[r], x_recv.at[r], at_x(1)).wait_send()
            send(total.at[r, :, rest, :], back.at[r, :, rest, :], b_send.at[r], b_recv.at[r, 0], at_x(1)).wait_send()

        c_copy(r).wait_send()
        p_copy(r).wait_send()
        return carry

    lax.fori_loop(0, Z, drain_rows, 0)
    for way in (0, 1):
        send(far_staged.at[way], far_back.at[way], f_send.at[way], f_recv.at[way, 0], partner).wait_send()
        send(total.at[half, far_chunks(way)], far_back.at[way], g_send.at[way], f_recv.at[way, 0], partner).wait_send()


def layer(mixed, tokens, gain, routes, shares, sgate, sup, sdown, gate, up, down):
    top = routes.shape[1]
    S, D = tokens.shape
    H = D // lax.axis_size("tp")
    X = ROW_RING
    Z = lax.axis_size("ep") // X
    nc = CHUNKS
    W = H // nc
    R = 16
    F = gate.shape[2]
    SF = sgate.shape[1]
    bf = jnp.bfloat16
    dma = pltpu.SemaphoreType.DMA
    vm = pl.BlockSpec(memory_space=pltpu.VMEM)
    hb = pl.BlockSpec(memory_space=pl.ANY)
    return pl.pallas_call(
        functools.partial(layer_kernel, (Z, X, S, H, R, nc, top)),
        out_shape=jax.ShapeDtypeStruct((S, H), bf),
        in_specs=[hb] * 11,
        out_specs=vm,
        scratch_shapes=[
            pltpu.VMEM((S, D), bf),
            pltpu.VMEM((1, D), jnp.float32),
            pltpu.VMEM((top, S), jnp.int32),
            pltpu.VMEM((top, S), jnp.float32),
            pltpu.VMEM((16, LANES), jnp.float32),
            pltpu.VMEM((S, D), bf),
            pltpu.VMEM((S, D), bf),
            pltpu.VMEM((S, D), bf),
            pltpu.VMEM((S, D), bf),
            pltpu.VMEM((D, 2 * SF), bf),
            pltpu.VMEM((SF, D), bf),
            pltpu.VMEM((S, SF), bf),
            pltpu.VMEM((2, S, H), bf),
            pltpu.VMEM((S, H), bf),
            pltpu.VMEM((Z, nc, S, W), bf),
            pltpu.VMEM((Z, 16, LANES), bf),
            pltpu.VMEM((Z, X * R, LANES), bf),
            pltpu.VMEM((Z, LANES, X * R), bf),
            pltpu.VMEM((Z, nc, X * R, W), bf),
            pltpu.VMEM((Z, 2, nc, X * R, W), bf),
            pltpu.VMEM((D, 2 * F), bf),
            pltpu.VMEM((F, D), bf),
            pltpu.VMEM((Z, 2, nc, X * R, W), bf),
            pltpu.VMEM((Z, nc, X * R, W), bf),
            pltpu.VMEM((Z, nc, X * R, W), bf),
            pltpu.VMEM((Z, nc, X * R, W), bf),
            pltpu.VMEM((Z + 1, nc, S, W), bf),
            pltpu.VMEM((Z, nc, S, W), bf),
            pltpu.VMEM((2, X * R, LANES), bf),
            pltpu.VMEM((2, LANES, X * R), bf),
            pltpu.VMEM((2, nc // 2, X * R, W), bf),
            pltpu.VMEM((2, nc // 2, X * R, W), bf),
            dma((12,)),
            dma((2,)),
            dma((2,)),
            dma((2, Z // 2)),
            dma((Z,)),
            dma((2, Z // 2, nc)),
            dma((Z, nc)),
            dma((Z,)),
            dma((Z,)),
            dma((Z,)),
            dma((Z,)),
            dma((Z,)),
            dma((Z,)),
            dma((Z,)),
            dma((Z, nc)),
            dma((Z, nc)),
            dma((Z + 1, nc)),
            dma((2,)),
            dma((2, nc // 2)),
            dma((2,)),
            pltpu.SemaphoreType.REGULAR,
            pltpu.SemaphoreType.REGULAR,
        ],
        compiler_params=pltpu.CompilerParams(
            collective_id=0, has_side_effects=True, vmem_limit_bytes=56300000
        ),
        name="layer",
    )(mixed, tokens, gain[None, :], routes.T, shares.T, sgate, sup, sdown, gate, up, down)


def mixer_kernel(
    tokens_hbm,
    prior_hbm,
    gain_hbm,
    weight_hbm,
    decay_hbm,
    freq_hbm,
    step_hbm,
    imap_hbm,
    omap_hbm,
    skip_hbm,
    project_hbm,
    mixed_hbm,
    state_hbm,
    tokens_ref,
    old,
    gain_ref,
    weight,
    decay_ref,
    freq_ref,
    step_ref,
    imap_ref,
    omap_ref,
    skip_ref,
    project,
    active_ref,
    mixed,
    fresh,
    in_sem,
    out_sem,
    mixed_sem,
):
    S, D = tokens_ref.shape
    width = weight.shape[1]
    groups, entries = decay_ref.shape
    members = width // groups
    f4, bf = jnp.float32, jnp.bfloat16
    lane_groups = LANES // entries
    block = LANES // members
    cols = block * entries

    fetched = {}
    for i, (name, src, dst) in enumerate(
        (
            ("tokens", tokens_hbm, tokens_ref),
            ("gain", gain_hbm, gain_ref),
            ("step", step_hbm, step_ref),
            ("decay", decay_hbm, decay_ref),
            ("freq", freq_hbm, freq_ref),
            ("weight", weight_hbm, weight),
            ("imap", imap_hbm, imap_ref),
            ("old", prior_hbm, old),
            ("skip", skip_hbm, skip_ref),
            ("omap", omap_hbm, omap_ref),
            ("project", project_hbm, project),
        )
    ):
        fetched[name] = pltpu.make_async_copy(src, dst, in_sem.at[i])
        fetched[name].start()

    def state_copy(part, q):
        lanes = pl.ds(q * cols, cols)
        return pltpu.make_async_copy(fresh.at[part, :, lanes], state_hbm.at[part, :, lanes], out_sem.at[part, q])

    for name in ("step", "decay", "freq"):
        fetched[name].wait()

    eye = lax.broadcasted_iota(jnp.int32, (groups, groups), 0) == lax.broadcasted_iota(jnp.int32, (groups, groups), 1)
    log_column = jnp.sum(jnp.where(eye, step_ref[...], 0.0), axis=1, keepdims=True)
    step_size = jnp.exp(log_column)
    real_rate = -decay_ref[...]
    frequency = freq_ref[...]
    magnitude = jnp.exp(real_rate * step_size)
    turn_real = magnitude * jnp.cos(frequency * step_size)
    turn_imag = magnitude * jnp.sin(frequency * step_size)
    denominator = real_rate * real_rate + frequency * frequency
    hold_real = ((turn_real - 1.0) * real_rate + turn_imag * frequency) / denominator
    hold_imag = (turn_imag * real_rate - (turn_real - 1.0) * frequency) / denominator
    doubled = [jnp.concatenate([v] * lane_groups, axis=1) for v in (turn_real, turn_imag, hold_real, hold_imag)]
    row_group = lax.broadcasted_iota(jnp.int32, (groups, LANES), 0)
    lane_group = lax.broadcasted_iota(jnp.int32, (groups, LANES), 1) // entries

    fetched["tokens"].wait()
    fetched["gain"].wait()
    values = tokens_ref[...].astype(f4)
    factor = lax.rsqrt(jnp.mean(values * values, axis=-1, keepdims=True) + norm_eps)
    normed = (values * factor * gain_ref[...]).astype(bf)
    fetched["weight"].wait()
    drive = jnp.dot(normed, weight[...], preferred_element_type=f4).astype(bf)
    for name in ("imap", "old", "skip", "omap"):
        fetched[name].wait()

    in_row = lax.broadcasted_iota(jnp.int32, (LANES, LANES), 0) // members
    in_lane = lax.broadcasted_iota(jnp.int32, (LANES, LANES), 1) // entries
    out_row = lax.broadcasted_iota(jnp.int32, (LANES, 2 * LANES), 0) // members
    out_lane = lax.broadcasted_iota(jnp.int32, (LANES, 2 * LANES), 1) // entries

    for q in range(width // LANES):
        channels = slice(q * LANES, (q + 1) * LANES)
        mine = drive[:, channels]
        maps = [jnp.concatenate([imap_ref[part, channels, :]] * lane_groups, axis=1) for part in range(2)]
        outs = [jnp.concatenate([omap_ref[part, channels, :]] * (2 * lane_groups), axis=1) for part in range(2)]
        readout = mine.astype(f4) * skip_ref[:, channels]
        for m in range(cols // LANES):
            mask = in_row == in_lane + m * lane_groups
            both = jnp.concatenate([jnp.where(mask, v, 0.0) for v in maps], axis=1).astype(bf)
            push = jnp.dot(mine, both, preferred_element_type=f4)
            push_real, push_imag = push[:, :LANES], push[:, LANES:]
            first = q * block + m * lane_groups
            tr, ti, hr, hi = [
                jnp.sum(jnp.where(row_group == lane_group + first, v, 0.0), axis=0, keepdims=True) for v in doubled
            ]
            at = slice(q * cols + m * LANES, q * cols + (m + 1) * LANES)
            old_real, old_imag = old[0, :, at], old[1, :, at]
            fresh[0, :, at] = tr * old_real - ti * old_imag + (push_real * hr - push_imag * hi)
            fresh[1, :, at] = tr * old_imag + ti * old_real + (push_real * hi + push_imag * hr)
        state_copy(0, q).start()
        state_copy(1, q).start()
        for h in range(cols // (2 * LANES)):
            at = slice(q * cols + h * 2 * LANES, q * cols + (h + 1) * 2 * LANES)
            mask = out_row == out_lane + h * 2 * lane_groups
            for part in range(2):
                spread_out = jnp.where(mask, outs[part] if part == 0 else -outs[part], 0.0).astype(bf)
                readout = readout + lax.dot_general(
                    fresh[part, :, at].astype(bf), spread_out, (((1,), (1,)), ((), ())), preferred_element_type=f4
                )
        active_ref[:, channels] = jax.nn.gelu(readout).astype(bf)
    fetched["project"].wait()
    quarter = D // 4
    sent = []
    for h in range(4):
        at = slice(h * quarter, (h + 1) * quarter)
        mixed[:, at] = jnp.dot(active_ref[...], project[:, at], preferred_element_type=f4).astype(bf)
        sent.append(pltpu.make_async_copy(mixed.at[:, at], mixed_hbm.at[:, at], mixed_sem.at[h]))
        sent[-1].start()
    for copy in sent:
        copy.wait()
    for q in range(width // LANES):
        for part in range(2):
            state_copy(part, q).wait()


def mixer(tokens, prior, gain, weight, decay, freq, log_step, imap, omap, skip, project):
    S, D = tokens.shape
    width = weight.shape[1]
    f4 = jnp.float32
    hb = pl.BlockSpec(memory_space=pl.ANY)
    dma = pltpu.SemaphoreType.DMA
    by_channel = (2, width, imap.shape[2])
    return pl.pallas_call(
        mixer_kernel,
        out_shape=(
            jax.ShapeDtypeStruct((S, D), jnp.bfloat16),
            jax.ShapeDtypeStruct(prior.shape, jnp.float32),
        ),
        in_specs=[hb] * 11,
        out_specs=(hb, hb),
        scratch_shapes=[
            pltpu.VMEM((S, D), tokens.dtype),
            pltpu.VMEM(prior.shape, f4),
            pltpu.VMEM((1, D), f4),
            pltpu.VMEM(weight.shape, weight.dtype),
            pltpu.VMEM(decay.shape, f4),
            pltpu.VMEM(freq.shape, f4),
            pltpu.VMEM((1, log_step.shape[0]), f4),
            pltpu.VMEM(by_channel, f4),
            pltpu.VMEM(by_channel, f4),
            pltpu.VMEM((1, width), f4),
            pltpu.VMEM(project.shape, project.dtype),
            pltpu.VMEM((S, width), tokens.dtype),
            pltpu.VMEM((S, D), tokens.dtype),
            pltpu.VMEM(prior.shape, f4),
            dma((11,)),
            dma((2, width // LANES)),
            dma((4,)),
        ],
        compiler_params=pltpu.CompilerParams(vmem_limit_bytes=VMEM_ALL),
        name="mixer",
    )(
        tokens,
        prior,
        gain[None, :],
        weight,
        decay,
        freq,
        log_step[None, :],
        jnp.swapaxes(imap, 2, 3).reshape(by_channel),
        omap.reshape(by_channel),
        skip[None, :],
        project,
    )


def body(
    tokens,
    prior_state,
    mix_gain,
    in_weight,
    decay_rate,
    frequency,
    log_step,
    input_map,
    output_map,
    skip_gain,
    out_weight,
    channel_gain,
    expert_gate,
    expert_up,
    expert_down,
    shared_gate,
    shared_up,
    shared_down,
    routes,
    route_weights,
):
    mixed, new_state = mixer(
        tokens,
        prior_state,
        mix_gain,
        in_weight,
        decay_rate,
        frequency,
        log_step,
        input_map,
        output_map,
        skip_gain,
        out_weight,
    )
    layer_out = layer(
        mixed,
        tokens,
        channel_gain,
        routes,
        route_weights,
        shared_gate,
        shared_up,
        shared_down,
        expert_gate,
        expert_up,
        expert_down,
    )
    return (layer_out, new_state)


def solution(mesh):
    in_specs = (
        P(("grp", "ep"), None),
        P(None, ("grp", "ep"), "tp"),
        P(),
        P(None, "tp"),
        P("tp", None),
        P("tp", None),
        P("tp"),
        P(None, "tp", None, None),
        P(None, "tp", None, None),
        P("tp"),
        P("tp", None),
        P(),
        P("ep", None, "tp"),
        P("ep", None, "tp"),
        P("ep", "tp", None),
        P(None, "tp"),
        P(None, "tp"),
        P("tp", None),
        P(("grp", "ep"), None),
        P(("grp", "ep"), None),
    )
    out_specs = (P(("grp", "ep"), "tp"), P(None, ("grp", "ep"), "tp"))
    return jax.shard_map(body, mesh=mesh, in_specs=in_specs, out_specs=out_specs, check_vma=False)
```
